32 devices in a mesh: rep: 2 (over y), fs: 4 (over z), tp: 4 (over x, core).
Axes of the slice: x: 2, y: 2, z: 4, core: 2. Of those that a mesh axis runs over, the one named last changes fastest.
Arguments:
- tokens: bfloat16 [2048, 2048], P(('rep', 'fs')), may hold values from -6 to 6
- mix_gain: float32 [2048], replicated, may hold values from 0.1 to 1.9
- group_weight: float32 [512, 2048], P('fs', 'tp'), may hold values from -0.25 to 0.25
- group_scale: float32 [1, 2048], P(None, 'tp'), may hold values from 0.5 to 2
- mlp_gain: float32 [2048], replicated, may hold values from 0.1 to 1.9
- up_weight: float32 [2048, 8192], P('fs', 'tp'), may hold values from -0.125 to 0.125
- up_scale: float32 [1, 8192], P(None, 'tp'), may hold values from 0.5 to 2
- down_weight: float32 [8192, 2048], P('tp', 'fs'), may hold values from -0.0625 to 0.0625
- down_scale: float32 [1, 2048], replicated, may hold values from 0.5 to 2
Outputs:
- layer_out: bfloat16 [2048, 2048], P(('rep', 'fs'))
The draws below stay inside these ranges and needn't reach their ends.
All inputs are finite; a program needn't handle non-finite values.
Results may differ from the reference program's by a relative error of at most 0.013.
Values may be sent and summed in bfloat16 or wider, within the bound.
A program may use at most 64 MiB of HBM per device.

```python
import math
import jax
import jax.numpy as jnp
from jax import lax

D = 2048
FF = 8192
GROUPS = 4
GROUP_DIM = 512
LENGTH = 128
TOKENS = 2048
N_TP = 4


def shard_levels(stream_key, dims, cuts, smallest, high):
    level, own = 1.0, jax.random.fold_in(stream_key, 6)
    for dim, blocks in cuts:
        steps = jnp.exp(jax.random.uniform(jax.random.fold_in(own, dim), (blocks,), jnp.float32, smallest / len(cuts), high / len(cuts)))
        level = level * jnp.repeat(steps, dims[dim] // blocks).reshape([-1 if axis == dim else 1 for axis in range(len(dims))])
    return level


def gaussian(rng, shape, spread, most, shards=(), kind=jnp.bfloat16):
    values = jax.random.normal(rng, shape, jnp.float32) * spread
    if len(shards) > 0:
        values = shard_levels(rng, shape, shards, -0.22, 0.18) * values
    return jnp.clip(values, min=-most, max=most).astype(kind)


def setup_inputs(seed: int = 0) -> dict:
    keys = jax.random.split(jax.random.key(seed), 10)
    tokens = gaussian(keys[0], (TOKENS, D), 1.0, 6.0, ((0, 8),))
    mix_gain = jnp.clip(1.0 + 0.18 * jax.random.normal(keys[1], (D,), jnp.float32), 0.1, 1.9)
    group_weight = gaussian(keys[2], (GROUP_DIM, D), GROUP_DIM ** -0.5, 0.25, ((0, 4), (1, 4)), jnp.float32)
    group_scale = jnp.clip(jnp.exp(math.log(2.0) - 1.3862944 * jax.random.uniform(keys[3], (1, D), jnp.float32) ** shard_levels(keys[3], (1, D), ((1, 4),), -0.2, 0.2)), 0.5, 2.0)
    mlp_gain = jnp.clip(1.0 + 0.18 * jax.random.normal(keys[4], (D,), jnp.float32), 0.1, 1.9)
    up_weight = gaussian(keys[5], (D, FF), D ** -0.5, 0.125, ((0, 4), (1, 4)), jnp.float32)
    up_scale = jnp.clip(jnp.exp(math.log(2.0) - 1.3862944 * jax.random.uniform(keys[6], (1, FF), jnp.float32) ** shard_levels(keys[6], (1, FF), ((1, 4),), -0.2, 0.2)), 0.5, 2.0)
    down_weight = gaussian(keys[7], (FF, D), FF ** -0.5, 0.0625, ((0, 4), (1, 4)), jnp.float32)
    down_scale = jnp.clip(jnp.exp(jax.random.uniform(keys[8], (1, D), jnp.float32, math.log(0.5), math.log(2.0))), 0.5, 2.0)
    return {"tokens": tokens, "mix_gain": mix_gain, "group_weight": group_weight, "group_scale": group_scale, "mlp_gain": mlp_gain, "up_weight": up_weight, "up_scale": up_scale, "down_weight": down_weight, "down_scale": down_scale}


norm_eps = 1e-06

def norm_rows(values, gain):
    promoted = values.astype(jnp.float32)
    inverse = lax.rsqrt(lax.optimization_barrier(jnp.mean(promoted * promoted, axis=-1, keepdims=True)) + norm_eps)
    return (promoted * inverse * gain.astype(jnp.float32)).astype(jnp.bfloat16)

def band_means(inputs, window, seq_length):
    row_count, columns = inputs.shape
    by_sequence = inputs.reshape(row_count // seq_length, seq_length, columns)
    position = jnp.arange(seq_length, dtype=jnp.int32)
    offset = position[:, None] - position[None, :]
    band_mask = ((offset >= 0) & (offset < window)).astype(jnp.float32)
    divisor = jnp.minimum(position + 1, window).astype(jnp.float32)
    summed = jnp.einsum('ts,nsc->ntc', band_mask, by_sequence, precision=lax.Precision.HIGHEST)
    return (summed / divisor[None, :, None] - by_sequence).reshape(row_count, columns)

def reference(tokens, mix_gain, group_weight, group_scale, mlp_gain, up_weight, up_scale, down_weight, down_scale):
    normed = norm_rows(tokens, mix_gain).astype(jnp.float32)
    pieces = []
    for group_index in range(GROUPS):
        first_col = group_index * GROUP_DIM
        inputs = normed[:, first_col:first_col + GROUP_DIM]
        pooled = band_means(inputs, 2 ** (group_index + 1), LENGTH).astype(jnp.bfloat16)
        weight_cols = group_weight[:, first_col:first_col + GROUP_DIM].astype(jnp.bfloat16)
        product = jnp.dot(pooled, weight_cols, preferred_element_type=jnp.float32)
        pieces.append(product * group_scale[:, first_col:first_col + GROUP_DIM])
    mixed_cols = jnp.concatenate(pieces, axis=1)
    carried = (tokens.astype(jnp.float32) + mixed_cols).astype(jnp.bfloat16)
    normed_mlp = norm_rows(carried, mlp_gain)
    pre_act = jnp.dot(normed_mlp, up_weight.astype(jnp.bfloat16), preferred_element_type=jnp.float32) * up_scale
    hidden = jnp.square(jax.nn.relu(pre_act)).astype(jnp.bfloat16)
    tp_block = FF // N_TP
    summed = jnp.zeros(carried.shape, jnp.float32)
    for tp_index in range(N_TP):
        rows_here = slice(tp_index * tp_block, (tp_index + 1) * tp_block)
        partial_value = jnp.dot(hidden[:, rows_here], down_weight[rows_here].astype(jnp.bfloat16), preferred_element_type=jnp.float32) * down_scale
        summed = summed + partial_value.astype(jnp.bfloat16).astype(jnp.float32)
    return (carried.astype(jnp.float32) + summed).astype(jnp.bfloat16)
```

```python
import functools

import jax
import jax.numpy as jnp
from jax import lax
from jax.experimental import pallas as pl
from jax.experimental.pallas import tpu as pltpu
from jax.sharding import PartitionSpec as P

GROUPS = 4
LENGTH = 128


norm_eps = 1e-06


def norm_rows(values, gain):
    promoted = values.astype(jnp.float32)
    inverse = lax.rsqrt(jnp.mean(promoted * promoted, axis=-1, keepdims=True) + norm_eps)
    return (promoted * inverse * gain).astype(jnp.bfloat16)


def band_means(inputs, window, seq_length):
    row_count, columns = inputs.shape
    by_sequence = inputs.reshape(row_count // seq_length, seq_length, columns)
    position = jnp.arange(seq_length, dtype=jnp.int32)
    offset = position[:, None] - position[None, :]
    band_mask = ((offset >= 0) & (offset < window)).astype(jnp.bfloat16)
    divisor = jnp.minimum(position + 1, window).astype(jnp.float32)
    summed = jnp.einsum("ts,nsc->ntc", band_mask, by_sequence, preferred_element_type=jnp.float32)
    return (summed / divisor[None, :, None] - by_sequence.astype(jnp.float32)).reshape(
        row_count, columns
    )


def body(
    tokens,
    mix_gain,
    group_weight,
    group_scale,
    mlp_gain,
    up_weight,
    up_scale,
    down_weight,
    down_scale,
):
    model_width = tokens.shape[1]
    group_width = model_width // GROUPS
    own_cols = group_weight.shape[1]
    column_start = lax.axis_index("tp") * own_cols
    group_index = column_start // group_width
    normed = norm_rows(tokens, mix_gain)
    inputs = lax.dynamic_slice_in_dim(normed, group_index * group_width, group_width, 1)
    window = jnp.left_shift(jnp.int32(2), group_index)
    pooled = band_means(inputs, window, LENGTH).astype(jnp.bfloat16)
    mixed_cols = (
        jnp.dot(
            pooled,
            lax.all_gather(group_weight.astype(jnp.bfloat16), "fs", axis=0, tiled=True),
            preferred_element_type=jnp.float32,
        )
        * group_scale
    )
    own_tokens = lax.dynamic_slice_in_dim(tokens, column_start, own_cols, 1)
    carried_cols = (own_tokens.astype(jnp.float32) + mixed_cols).astype(jnp.bfloat16)
    carried = lax.all_gather(carried_cols, "tp", axis=1, tiled=True)
    normed_mlp = norm_rows(carried, mlp_gain)
    pre_act = (
        jnp.dot(
            normed_mlp,
            lax.all_gather(up_weight.astype(jnp.bfloat16), "fs", axis=0, tiled=True),
            preferred_element_type=jnp.float32,
        )
        * up_scale
    )
    hidden = jnp.square(jax.nn.relu(pre_act)).astype(jnp.bfloat16)
    partial_value = (
        jnp.dot(
            hidden,
            lax.all_gather(down_weight.astype(jnp.bfloat16), "fs", axis=1, tiled=True),
            preferred_element_type=jnp.float32,
        )
        * down_scale
    )
    summed = lax.psum(partial_value.astype(jnp.bfloat16), "tp").astype(jnp.float32)
    return (carried.astype(jnp.float32) + summed).astype(jnp.bfloat16)


MESH = pl.DeviceIdType.MESH
CHUNKS = 4
PARTS = 2


def ring_kernel(
    sizes,
    tok_h, mg, gw_h, gs, lg, up_h, us, dn_h, ds,
    out_h,
    tok, gwf, upf, upo, dnf, dno,
    gwg, ups, upg, dns, dng,
    car, xn, hid, pb, ra, sx, rb, sz, ri, rc, og,
    ld, sw, rw, sy, ry, swu, rwu, syu, ryu, swd, rwd, syd, ryd, scz, rcz, scx, rcx, scc, rcc,
    sa, ra_s, sb, rb_s, st, rt, sm, rm, so, ro, wr,
):
    Z, T, C, rows, D, own, hg, hu, hd, fsub, dsub = sizes
    cw = dsub // C
    r, z, t = lax.axis_index("rep"), lax.axis_index("fs"), lax.axis_index("tp")
    cp = t + 1 - 2 * lax.rem(t, 2)
    xp = lax.rem(t + 2, T)
    cxp = lax.rem(cp + 2, T)
    peer_r = 1 - r
    bf, f32 = jnp.bfloat16, jnp.float32
    mate = z + 1 - 2 * lax.rem(z, 2)
    zk = (z, mate, lax.rem(z + 2, Z), Z - 1 - z)
    inner = (z > 0) & (z < Z - 1)
    outer = (z == 0) | (z == Z - 1)

    def mul(i, n):
        return pl.multiple_of(i * n, n)

    loads = {}

    def load(key, src, dst, k):
        c = pltpu.make_async_copy(src, dst, ld.at[k])
        c.start()
        loads[key] = c

    def load_up(k):
        load(("up", k), up_h.at[pl.ds(mul(r, hu), hu), pl.ds(mul(zk[k], fsub), fsub)], upf.at[k], 2 + k)

    def load_dn(k):
        load(("dn", k), dn_h.at[pl.ds(pl.multiple_of(zk[k] * 2 * hd + r * hd, hd), hd), :], dnf.at[k], 2 + Z + k)

    load("gw", gw_h, gwf, 0)
    load_up(2)
    load("tok", tok_h, tok, 1)
    load_up(3)
    load_up(1)
    load_up(0)
    load("upo", up_h.at[pl.ds(mul(peer_r, hu), hu), pl.ds(mul(z, fsub), fsub)], upo, 2 + 2 * Z)
    for k in (2, 3, 1, 0):
        load_dn(k)
    load("dno", dn_h.at[pl.ds(pl.multiple_of(z * 2 * hd + peer_r * hd, hd), hd), :], dno, 3 + 2 * Z)

    barrier = pltpu.get_barrier_semaphore()
    peers = [(r, zk[k], t) for k in range(1, Z)] + [(peer_r, z, t), (r, z, xp), (r, z, cp)]
    for p in peers:
        pl.semaphore_signal(barrier, inc=1, device_id=p, device_id_type=MESH)
    loads["gw"].wait()
    gwg[pl.ds(mul(z, 2 * hg), 2 * hg), :] = gwf[...].astype(bf)
    loads[("up", 2)].wait()
    ups[2] = upf[2].astype(bf)
    with jax.named_scope("barrier"):
        pl.semaphore_wait(barrier, len(peers))

    sends = []

    def remote(src, dst, ss, rs, dev):
        return pltpu.make_async_remote_copy(
            src_ref=src, dst_ref=dst, send_sem=ss, recv_sem=rs, device_id=dev, device_id_type=MESH
        )

    role = [None]

    def guarded(fn, when=None):
        for p in (role[0],):
            if p is not None:
                when = p if when is None else when & p
        if when is None:
            fn()
        else:
            pl.when(when)(fn)
        return when

    def send(src, dst, ss, rs, dev, when=None):
        when = guarded(lambda: remote(src, dst, ss, rs, dev).start(), when)
        sends.append((when, (src, dst, ss, rs, dev)))

    def drain():
        for when, args in sends:
            if when is None:
                remote(*args).wait_send()
            else:
                pl.when(when)(lambda args=args: remote(*args).wait_send())

    def got(dst, ss, rs):
        guarded(lambda: remote(dst, dst, ss, rs, (peer_r, z, t)).wait_recv())

    def only(who, *steps):
        role[0] = who
        for name, fn, *args in steps:
            run(name, fn, *args)
        role[0] = None

    def run(name, fn, *args):
        with jax.named_scope(name + "".join(map(str, [a for a in args if isinstance(a, int)]))):
            fn(*args)

    def gw_at(src, rep):
        return gwg.at[pl.ds(pl.multiple_of(src * 2 * hg + rep * hg, hg), hg), :]

    pu = hu // PARTS

    def up_at(src, rep, i):
        return upg.at[pl.ds(pl.multiple_of(src * 2 * hu + rep * hu + i * pu, pu), pu), :]

    def dn_at(c, src, rep):
        return dng.at[c, pl.ds(mul(rep, hd), hd), pl.ds(mul(src, cw), cw)]

    def up_send(k, when=None):
        for i in range(PARTS):
            piece = ups.at[k, pl.ds(i * pu, pu)]
            send(piece, up_at(z, r, i), swu.at[k, i], rwu.at[z, i], (r, zk[k], t), when)

    def dn_send(c, k, when=None):
        send(dns.at[k, c], dn_at(c, z, r), swd.at[c, k], rwd.at[c, z], (r, zk[k], t), when)

    for k in (3, 2, 1):
        send(gw_at(z, r), gw_at(z, r), sw.at[k], rw.at[z], (r, zk[k], t))
    loads[("up", 3)].wait()
    ups[3] = upf[3].astype(bf)
    loads[("up", 1)].wait()
    ups[1] = upf[1].astype(bf)
    up_send(2, inner)
    up_send(3, inner)
    up_send(1)

    loads["tok"].wait()
    full = tok[...].astype(f32)
    inv = lax.rsqrt(jnp.mean(full * full, axis=-1, keepdims=True) + norm_eps)
    cols = pl.ds(mul(t, own), own)
    mine = tok[:, cols].astype(f32)
    normed = (mine * inv * mg[:, cols]).astype(bf)
    window = jnp.left_shift(jnp.int32(2), t)
    ti = lax.broadcasted_iota(jnp.int32, (LENGTH, LENGTH), 0)
    si = lax.broadcasted_iota(jnp.int32, (LENGTH, LENGTH), 1)
    band = jnp.where((ti - si >= 0) & (ti - si < window), 1.0, 0.0).astype(bf)
    pos = lax.broadcasted_iota(jnp.int32, (LENGTH, own), 0)
    divisor = jnp.minimum(pos + 1, window).astype(f32)
    for s in range(rows // LENGTH):
        part = normed[s * LENGTH:(s + 1) * LENGTH]
        summed = jnp.dot(band, part, preferred_element_type=f32)
        xn[s * LENGTH:(s + 1) * LENGTH, :own] = (summed / divisor - part.astype(f32)).astype(bf)

    def gw_swap(src):
        got(gw_at(src, r), sw.at[0], rw.at[src])
        send(gw_at(src, r), gw_at(src, r), sy.at[src], ry.at[src], (peer_r, z, t))

    def up_swap(src):
        for i in range(PARTS):
            b = up_at(src, r, i)
            got(b, swu.at[0, i], rwu.at[src, i])
            send(b, b, syu.at[src, i], ryu.at[src, i], (peer_r, z, t))

    def up_swapped(src):
        for i in range(PARTS):
            got(up_at(src, peer_r, i), syu.at[src, i], ryu.at[src, i])

    for k in (3, 2):
        loads[("dn", k)].wait()
        dns[k, 0] = dnf[k, :, :cw].astype(bf)
    with jax.named_scope("gwswap"):
        gw_swap(zk[1])
        for k in (2, 3):
            gw_swap(zk[k])
        up_send(3, outer)
        up_send(2, outer)
        dn_send(0, 3, outer)
        dn_send(0, 2, outer)
    with jax.named_scope("gwswapped"):
        for k in (1, 2, 3):
            got(gw_at(zk[k], peer_r), sy.at[zk[k]], ry.at[zk[k]])
    with jax.named_scope("mix"):
        mixed = jnp.dot(xn[:, :own], gwg[...], preferred_element_type=f32) * gs[...]
        car[z, t] = (tok[:, cols].astype(f32) + mixed).astype(bf)
    H = rows // LENGTH
    hr = LENGTH
    low = 1 - lax.div(z, Z // 2)
    near, far = 1 + low, 3 * low
    blocks = (z, mate, near, far)
    def half(h):
        return pl.ds(h * hr, hr)

    def to_x(src, h):
        b = car.at[src, t, half(h)]
        send(b, b, scx.at[src, h], rcx.at[src, h], (r, z, xp))

    def to_core(src, h, q, k):
        b = car.at[src, q, half(h)]
        send(b, b, scc.at[src, k, h], rcc.at[src, k, h], (r, z, cp))

    def to_z(src, h, when_up, when_down):
        b = car.at[src, t, half(h)]
        send(b, b, scz.at[0, src, h], rcz.at[src, h], (r, lax.rem(z + 1, Z), t), when_up)
        send(b, b, scz.at[1, src, h], rcz.at[src, h], (r, lax.rem(z + Z - 1, Z), t), when_down)

    for h in range(H):
        to_z(z, h, z < Z - 1, z > 0)
        to_x(z, h)
        to_core(z, h, t, 0)
    with jax.named_scope("casts"):
        for k in (2, 3, 1):
            if k == 1:
                loads[("dn", 1)].wait()
            for c in range(int(k != 1), C):
                dns[k, c] = dnf[k, :, c * cw:(c + 1) * cw].astype(bf)
        loads[("up", 0)].wait()
        upg[pl.ds(pl.multiple_of(z * 2 * hu + r * hu, hu), hu), :] = upf[0].astype(bf)
        loads["upo"].wait()
        upg[pl.ds(pl.multiple_of(z * 2 * hu + peer_r * hu, hu), hu), :] = upo[...].astype(bf)
        loads[("dn", 0)].wait()
        loads["dno"].wait()
        for c in range(C):
            here = pl.ds(mul(z, cw), cw)
            dng[c, pl.ds(mul(r, hd), hd), here] = dnf[0, :, c * cw:(c + 1) * cw].astype(bf)
            dng[c, pl.ds(mul(peer_r, hd), hd), here] = dno[:, c * cw:(c + 1) * cw].astype(bf)

    def arrive(d, h):
        src = blocks[d]
        got(car.at[src, t, half(h)], scz.at[0, src, h], rcz.at[src, h])
        to_z(src, h, (src < z) & (z < Z - 1), (src > z) & (z > 0))
        to_x(src, h)
        to_core(src, h, t, 0)

    def from_x(d, h):
        src = blocks[d]
        got(car.at[src, xp, half(h)], scx.at[src, h], rcx.at[src, h])
        to_core(src, h, xp, 1)

    def dn_group(*pieces):
        for c, k in pieces:
            dn_send(c, k)

    def dn_outer(c):
        dn_group((c, 3), (c, 2), (c, 1))

    def dn_early():
        dn_group((0, 3), (1, 3))

    def dn_rest():
        dn_group((2, 3), (1, 1))

    def far_core():
        for h in range(H):
            got(car.at[far, cp, half(h)], scc.at[far, 0, h], rcc.at[far, 0, h])

    def dn_forward(c, k):
        src = zk[k]
        got(dn_at(c, src, r), swd.at[c, k], rwd.at[c, src])
        send(dn_at(c, src, r), dn_at(c, src, r), syd.at[c, k], ryd.at[c, src], (peer_r, z, t))

    def up(d):
        src = blocks[d]
        for h in range(H):
            hs = half(h)
            if d < 3:
                got(car.at[src, cp, hs], scc.at[src, 0, h], rcc.at[src, 0, h])
            got(car.at[src, cxp, hs], scc.at[src, 1, h], rcc.at[src, 1, h])
        total = jnp.zeros((rows, 1), f32)
        for q in range(T):
            c = car[src, q].astype(f32)
            total += jnp.sum(c * c, axis=-1, keepdims=True)
        scale = lax.rsqrt(total / D + norm_eps)
        for q in range(T):
            part = slice(q * own, (q + 1) * own)
            xn[:, part] = (car[src, q].astype(f32) * scale * lg[:, part]).astype(bf)
        pre = jnp.dot(xn[...], upg[...], preferred_element_type=f32)
        pre = jnp.maximum(pre * us[:, pl.ds(mul(z, fsub), fsub)], 0.0)
        hid[src] = (pre * pre).astype(bf)

    def dn_ready(c):
        for k in range(1, Z):
            src = zk[k]
            got(dn_at(c, src, peer_r), syd.at[c, k], ryd.at[c, src])

    def down(c, k):
        src = zk[k]
        p = jnp.dot(hid[src], dng[c], preferred_element_type=f32)
        for q in range(T):
            part = p[:, q * cw:(q + 1) * cw] * ds[:, q * own + c * cw:q * own + (c + 1) * cw]
            pb[c, src, q] = part.astype(bf)
        for j, q in ((1, cxp), (0, cp)):
            send(pb.at[c, src, q], ra.at[c, src, j], sa.at[c, src, j], ra_s.at[c, src, j], (r, z, cp))

    def over_x(c, k):
        src = zk[k]
        got(ra.at[c, src, 1], sa.at[c, src, 1], ra_s.at[c, src, 1])
        sx[c, src] = (pb[c, src, xp].astype(f32) + ra[c, src, 1].astype(f32)).astype(bf)
        send(sx.at[c, src], rb.at[c, src], sb.at[c, src], rb_s.at[c, src], (r, z, xp))

    def both(c, src):
        return pb[c, src, t].astype(f32) + ra[c, src, 0].astype(f32) + rb[c, src].astype(f32)

    def joined(c, k):
        src = zk[k]
        got(ra.at[c, src, 0], sa.at[c, src, 0], ra_s.at[c, src, 0])
        got(rb.at[c, src], sb.at[c, src], rb_s.at[c, src])

    def to_inner(c, k):
        src = zk[k]
        joined(c, k)

        @pl.when(outer)
        def _():
            sz[c, src] = both(c, src).astype(bf)

        send(sz.at[c, src], ri.at[c, src], sm.at[c, src], rm.at[c, src], (r, mate, t), outer)

    def across(c, k):
        src = zk[k]

        @pl.when(inner)
        def _():
            got(ri.at[c, src], sm.at[c, src], rm.at[c, src])
            sz[c, src] = (both(c, src) + ri[c, src].astype(f32)).astype(bf)

        send(sz.at[c, src], rc.at[c, 1], st.at[c, src], rt.at[c, 1], (r, src, t), inner)

    def to_mate(c):
        joined(c, 1)
        sz[c, mate] = both(c, mate).astype(bf)
        send(sz.at[c, mate], rc.at[c, 0], st.at[c, mate], rt.at[c, 0], (r, mate, t))

    writes = []

    def write(c, q, j):
        cc = pltpu.make_async_copy(
            og.at[c, q], out_h.at[:, pl.ds(pl.multiple_of(q * own + c * cw, cw), cw)], wr.at[c, j]
        )
        cc.start()
        writes.append(cc)

    def pass_on(c, q, j, dev):
        b = og.at[c, q]
        send(b, b, so.at[c, j], ro.at[c, j], dev)

    def finish(c):
        joined(c, 0)
        acc = both(c, z) + car[z, t, :, :].astype(f32)[:, c * cw:(c + 1) * cw]
        for j in range(2):
            got(rc.at[c, j], st.at[c, z], rt.at[c, j])
            acc += rc[c, j].astype(f32)
        og[c, t] = acc.astype(bf)
        pass_on(c, t, 0, (r, z, xp))
        pass_on(c, t, 1, (r, z, cp))
        write(c, t, 0)

    def spread(c):
        got(og.at[c, xp], so.at[c, 0], ro.at[c, 0])
        pass_on(c, xp, 2, (r, z, cp))
        write(c, xp, 1)

    def collect(c):
        got(og.at[c, cp], so.at[c, 1], ro.at[c, 1])
        write(c, cp, 2)
        got(og.at[c, cxp], so.at[c, 2], ro.at[c, 2])
        write(c, cxp, 3)

    def up_ready():
        for k in (1, 2, 3):
            up_swapped(zk[k])

    run("us1", up_swap, zk[1])
    for h in range(H):
        run("fx", from_x, 0, h)
    only(outer, ("ous3", up_swap, zk[3]))
    only(inner, ("ius2", up_swap, zk[2]))
    for h in range(H):
        run("arr", arrive, 1, h)
    only(inner, ("dn", dn_early), ("ius3", up_swap, zk[3]), ("ifwd", dn_forward, 0, 2))
    for h in range(H):
        run("fx", from_x, 1, h)
    only(outer, ("ous2", up_swap, zk[2]))
    for h in range(H):
        run("arr", arrive, 2, h)
    only(outer, ("dn", dn_group, (0, 1)), ("ofwd", dn_forward, 0, 3))
    run("usd", up_ready)
    for h in range(H):
        run("fx", from_x, 2, h)
    run("up", up, 0)
    run("up", up, 1)
    for h in range(H):
        run("arr", arrive, 3, h)
    only(inner, ("dn", dn_group, (0, 1)))
    run("up", up, 2)
    for h in range(H):
        run("fx", from_x, 3, h)
    only(inner, ("dn", dn_rest))
    run("far", far_core)
    only(outer, ("dn", dn_group, (1, 3), (1, 2), (1, 1)))
    run("fwd", dn_forward, 0, 1)
    only(inner, ("ifwd", dn_forward, 0, 3), ("dn", dn_group, (0, 2), (1, 2)))
    only(outer, ("ofwd", dn_forward, 0, 2))
    run("up", up, 3)

    def forward(c):
        for k in (1, 2, 3):
            run("fwd", dn_forward, c, k)

    only(outer, ("dn", dn_outer, 2))
    only(inner, ("dn", dn_group, (2, 2), (2, 1), (3, 3)))
    for c in range(C):
        run("ready", dn_ready, c)
        for k in (3, 2, 1, 0):
            run("down", down, c, k)
        if c > 0:
            for k in (3, 2):
                run("inner", to_inner, c - 1, k)
        for k in (3, 2, 1, 0):
            run("x", over_x, c, k)
        if c == 0:
            forward(1)
            only(outer, ("dn", dn_outer, 3))
            only(inner, ("dn", dn_group, (3, 2), (3, 1)))
        if c + 2 < C:
            forward(c + 2)
        if c > 0:
            run("mate", to_mate, c - 1)
            for k in (3, 2):
                run("across", across, c - 1, k)
        if c > 1:
            run("fin", finish, c - 2)
    for k in (3, 2):
        run("inner", to_inner, C - 1, k)
    for c in range(C - 2):
        run("spread", spread, c)
    for k in (3, 2):
        run("across", across, C - 1, k)
    run("mate", to_mate, C - 1)
    run("fin", finish, C - 2)
    for c in range(C - 2):
        run("coll", collect, c)
    run("fin", finish, C - 1)
    for c in (C - 2, C - 1):
        run("spread", spread, c)
    for c in (C - 2, C - 1):
        run("coll", collect, c)
    with jax.named_scope("drain"):
        drain()
        for c in writes:
            c.wait()


def fused(mesh_shape, tokens, mix_gain, group_weight, group_scale, mlp_gain, up_weight, up_scale, down_weight, down_scale):
    Z, T = mesh_shape["fs"], mesh_shape["tp"]
    C = CHUNKS
    rows, D = tokens.shape
    own = group_weight.shape[1]
    hg, hu = group_weight.shape[0] // 2, up_weight.shape[0] // 2
    fsub = up_weight.shape[1] // Z
    hd = fsub // 2
    dsub = down_weight.shape[1]
    cw = dsub // C
    bf, f32 = jnp.bfloat16, jnp.float32
    dma = pltpu.SemaphoreType.DMA
    vm = pl.BlockSpec(memory_space=pltpu.VMEM)
    hbm = pl.BlockSpec(memory_space=pl.ANY)
    sizes = (Z, T, C, rows, D, own, hg, hu, hd, fsub, dsub)
    V = pltpu.VMEM
    H = rows // LENGTH
    piece = (C, Z, rows, cw)
    return pl.pallas_call(
        functools.partial(ring_kernel, sizes),
        out_shape=jax.ShapeDtypeStruct((rows, D), bf),
        in_specs=[hbm, vm, hbm, vm, vm, hbm, vm, hbm, vm],
        out_specs=hbm,
        scratch_shapes=[
            V((rows, D), bf), V((2 * hg, own), f32),
            V((Z, hu, fsub), f32), V((hu, fsub), f32), V((Z, hd, dsub), f32), V((hd, dsub), f32),
            V((Z * 2 * hg, own), bf), V((Z, hu, fsub), bf), V((Z * 2 * hu, fsub), bf),
            V((Z, C, hd, cw), bf), V((C, 2 * hd, Z * cw), bf),
            V((Z, T, rows, own), bf), V((rows, D), bf), V((Z, rows, fsub), bf), V((C, Z, T, rows, cw), bf),
            V((C, Z, 2, rows, cw), bf), V(piece, bf), V(piece, bf), V(piece, bf), V(piece, bf),
            V((C, 2, rows, cw), bf), V((C, T, rows, cw), bf),
            dma((4 + 2 * Z,)), dma((Z,)), dma((Z,)), dma((Z,)), dma((Z,)),
            dma((Z, PARTS)), dma((Z, PARTS)), dma((Z, PARTS)), dma((Z, PARTS)),
            dma((C, Z)), dma((C, Z)), dma((C, Z)), dma((C, Z)),
            dma((2, Z, H)), dma((Z, H)), dma((Z, H)), dma((Z, H)), dma((Z, 2, H)), dma((Z, 2, H)),
            dma((C, Z, 2)), dma((C, Z, 2)), dma((C, Z)), dma((C, Z)), dma((C, Z)), dma((C, 2)),
            dma((C, Z)), dma((C, Z)), dma((C, 3)), dma((C, 3)), dma((C, 4)),
        ],
        compiler_params=pltpu.CompilerParams(
            collective_id=0, has_side_effects=True, vmem_limit_bytes=60 * 1024 * 1024
        ),
    )(
        tokens, mix_gain[None], group_weight, group_scale, mlp_gain[None],
        up_weight, up_scale, down_weight, down_scale,
    )


def fits(mesh):
    shape = mesh.shape
    return shape["rep"] == 2 and shape["tp"] == GROUPS and shape["fs"] == shape["tp"]


def solution(mesh):
    in_specs = (
        P(("rep", "fs"), None),
        P(),
        P("fs", "tp"),
        P(None, "tp"),
        P(),
        P("fs", "tp"),
        P(None, "tp"),
        P("tp", "fs"),
        P(),
    )
    out_specs = P(("rep", "fs"), None)
    chosen = functools.partial(fused, mesh.shape) if fits(mesh) else body
    return jax.shard_map(chosen, mesh=mesh, in_specs=in_specs, out_specs=out_specs, check_vma=False)
```

```python
import functools

import jax
import jax.numpy as jnp
from jax import lax
from jax.experimental import pallas as pl
from jax.experimental.pallas import tpu as pltpu
from jax.sharding import PartitionSpec as P

GROUPS = 4
LENGTH = 128


norm_eps = 1e-06


def norm_rows(values, gain):
    promoted = values.astype(jnp.float32)
    inverse = lax.rsqrt(jnp.mean(promoted * promoted, axis=-1, keepdims=True) + norm_eps)
    return (promoted * inverse * gain).astype(jnp.bfloat16)


def band_means(inputs, window, seq_length):
    row_count, columns = inputs.shape
    by_sequence = inputs.reshape(row_count // seq_length, seq_length, columns)
    position = jnp.arange(seq_length, dtype=jnp.int32)
    offset = position[:, None] - position[None, :]
    band_mask = ((offset >= 0) & (offset < window)).astype(jnp.bfloat16)
    divisor = jnp.minimum(position + 1, window).astype(jnp.float32)
    summed = jnp.einsum("ts,nsc->ntc", band_mask, by_sequence, preferred_element_type=jnp.float32)
    return (summed / divisor[None, :, None] - by_sequence.astype(jnp.float32)).reshape(
        row_count, columns
    )


def body(
    tokens,
    mix_gain,
    group_weight,
    group_scale,
    mlp_gain,
    up_weight,
    up_scale,
    down_weight,
    down_scale,
):
    model_width = tokens.shape[1]
    group_width = model_width // GROUPS
    own_cols = group_weight.shape[1]
    column_start = lax.axis_index("tp") * own_cols
    group_index = column_start // group_width
    normed = norm_rows(tokens, mix_gain)
    inputs = lax.dynamic_slice_in_dim(normed, group_index * group_width, group_width, 1)
    window = jnp.left_shift(jnp.int32(2), group_index)
    pooled = band_means(inputs, window, LENGTH).astype(jnp.bfloat16)
    mixed_cols = (
        jnp.dot(
            pooled,
            lax.all_gather(group_weight.astype(jnp.bfloat16), "fs", axis=0, tiled=True),
            preferred_element_type=jnp.float32,
        )
        * group_scale
    )
    own_tokens = lax.dynamic_slice_in_dim(tokens, column_start, own_cols, 1)
    carried_cols = (own_tokens.astype(jnp.float32) + mixed_cols).astype(jnp.bfloat16)
    carried = lax.all_gather(carried_cols, "tp", axis=1, tiled=True)
    normed_mlp = norm_rows(carried, mlp_gain)
    pre_act = (
        jnp.dot(
            normed_mlp,
            lax.all_gather(up_weight.astype(jnp.bfloat16), "fs", axis=0, tiled=True),
            preferred_element_type=jnp.float32,
        )
        * up_scale
    )
    hidden = jnp.square(jax.nn.relu(pre_act)).astype(jnp.bfloat16)
    partial_value = (
        jnp.dot(
            hidden,
            lax.all_gather(down_weight.astype(jnp.bfloat16), "fs", axis=1, tiled=True),
            preferred_element_type=jnp.float32,
        )
        * down_scale
    )
    summed = lax.psum(partial_value.astype(jnp.bfloat16), "tp").astype(jnp.float32)
    return (carried.astype(jnp.float32) + summed).astype(jnp.bfloat16)


MESH = pl.DeviceIdType.MESH
CHUNKS = 4
PARTS = 4


def ring_kernel(
    sizes,
    tok_h, mg, gw_h, gs, lg, up_h, us, dn_h, ds,
    out_h,
    tok, gwf, upf, upo, dnf, dno,
    gwg, ups, upg, dns, dng,
    car, xn, hid, pb, ra, sx, rb, sz, ri, rc, og,
    ld, sent, rw, ry, rwu, ryu, rwd, ryd, rcz, rcx, rcc, rx, rj, rb_s, rt, rm, ro, rq,
):
    Z, T, C, rows, D, own, hg, hu, hd, fsub, dsub = sizes
    cw = dsub // C
    r, z, t = lax.axis_index("rep"), lax.axis_index("fs"), lax.axis_index("tp")
    cp = t + 1 - 2 * lax.rem(t, 2)
    xp = lax.rem(t + 2, T)
    cxp = lax.rem(cp + 2, T)
    peer_r = 1 - r
    bf, f32 = jnp.bfloat16, jnp.float32
    mate = z + 1 - 2 * lax.rem(z, 2)
    zk = (z, mate, lax.rem(z + 2, Z), Z - 1 - z)
    inner = (z > 0) & (z < Z - 1)
    outer = (z == 0) | (z == Z - 1)

    def mul(i, n):
        return pl.multiple_of(i * n, n)

    loads = {}

    def load(key, src, dst, k):
        c = pltpu.make_async_copy(src, dst, ld.at[k])
        c.start()
        loads[key] = c

    def load_up(k):
        load(("up", k), up_h.at[pl.ds(mul(r, hu), hu), pl.ds(mul(zk[k], fsub), fsub)], upf.at[k], 2 + k)

    def load_dn(k):
        load(("dn", k), dn_h.at[pl.ds(pl.multiple_of(zk[k] * 2 * hd + r * hd, hd), hd), :], dnf.at[k], 2 + Z + k)

    load("gw", gw_h, gwf, 0)
    load_up(2)
    load("tok", tok_h, tok, 1)
    load_up(3)
    load_up(1)
    load_up(0)
    load("upo", up_h.at[pl.ds(mul(peer_r, hu), hu), pl.ds(mul(z, fsub), fsub)], upo, 2 + 2 * Z)
    for k in (2, 3, 1, 0):
        load_dn(k)
    load("dno", dn_h.at[pl.ds(pl.multiple_of(z * 2 * hd + peer_r * hd, hd), hd), :], dno, 3 + 2 * Z)

    barrier = pltpu.get_barrier_semaphore()
    peers = [(r, zk[k], t) for k in range(1, Z)] + [(peer_r, z, t), (r, z, xp), (r, z, cp)]
    for p in peers:
        pl.semaphore_signal(barrier, inc=1, device_id=p, device_id_type=MESH)
    loads["gw"].wait()
    gwg[pl.ds(mul(z, 2 * hg), 2 * hg), :] = gwf[...].astype(bf)
    loads[("up", 2)].wait()
    ups[2] = upf[2].astype(bf)
    with jax.named_scope("barrier"):
        pl.semaphore_wait(barrier, len(peers))

    def remote(src, dst, ss, rs, dev):
        return pltpu.make_async_remote_copy(
            src_ref=src, dst_ref=dst, send_sem=ss, recv_sem=rs, device_id=dev, device_id_type=MESH
        )

    role = [None]

    def guarded(fn, when=None):
        for p in (role[0],):
            if p is not None:
                when = p if when is None else when & p
        if when is None:
            fn()
        else:
            pl.when(when)(fn)
        return when

    groups = ("gw", "gwy", "up", "upy", "dn", "dny", "carz", "carx", "carc", "pb", "sx", "sz", "og")

    def send(src, dst, group, rs, dev, when=None):
        guarded(lambda: remote(src, dst, sent.at[groups.index(group)], rs, dev).start(), when)

    def drain():
        three = pl.ds(1, Z - 1)
        same = (
            gwg.at[pl.ds(0, (Z - 1) * hg)], gwg.at[pl.ds(0, (Z - 1) * hg)], ups.at[three], ups.at[three],
            dns.at[three], dns.at[three], car.at[0, three], car.at[0], car.at[pl.ds(0, 2)],
            ra, rb, og.at[:, three], og.at[:, three],
        )
        for i, ref in enumerate(same):
            remote(ref, ref, sent.at[i], rcc.at[0], (peer_r, z, t)).wait_send()
        pltpu.make_async_copy(out_h, out_h, sent.at[len(same)]).wait()

    def got(dst, rs):
        guarded(lambda: remote(dst, dst, sent.at[0], rs, (peer_r, z, t)).wait_recv())

    def only(who, *steps):
        role[0] = who
        for name, fn, *args in steps:
            run(name, fn, *args)
        role[0] = None

    def run(name, fn, *args):
        with jax.named_scope(name + "".join(map(str, [a for a in args if isinstance(a, int)]))):
            fn(*args)

    def gw_at(src, rep):
        return gwg.at[pl.ds(pl.multiple_of(src * 2 * hg + rep * hg, hg), hg), :]

    pu = hu // PARTS

    def up_at(src, rep, i):
        return upg.at[pl.ds(pl.multiple_of(src * 2 * hu + rep * hu + i * pu, pu), pu), :]

    def dn_at(c, src, rep):
        return dng.at[c, pl.ds(mul(rep, hd), hd), pl.ds(mul(src, cw), cw)]

    early, late = range(PARTS // 2), range(PARTS // 2, PARTS)
    whole = range(PARTS)

    def up_send(k, when=None, parts=whole):
        for i in parts:
            piece = ups.at[k, pl.ds(i * pu, pu)]
            send(piece, up_at(z, r, i), "up", rwu.at[k - 1, i], (r, zk[k], t), when)

    def dn_send(c, k):
        send(dns.at[k, c], dn_at(c, z, r), "dn", rwd.at[k - 1, c], (r, zk[k], t))

    for k in (3, 2, 1):
        send(gw_at(z, r), gw_at(z, r), "gw", rw.at[k - 1], (r, zk[k], t))
    loads[("up", 1)].wait()
    ups[1] = upf[1].astype(bf)
    loads[("up", 3)].wait()
    ups[3] = upf[3].astype(bf)
    up_send(1, None, early)
    up_send(1, inner, late)

    loads["tok"].wait()
    full = tok[...].astype(f32)
    inv = lax.rsqrt(jnp.mean(full * full, axis=-1, keepdims=True) + norm_eps)
    cols = pl.ds(mul(t, own), own)
    mine = tok[:, cols].astype(f32)
    normed = (mine * inv * mg[:, cols]).astype(bf)
    window = jnp.left_shift(jnp.int32(2), t)
    ti = lax.broadcasted_iota(jnp.int32, (LENGTH, LENGTH), 0)
    si = lax.broadcasted_iota(jnp.int32, (LENGTH, LENGTH), 1)
    band = jnp.where((ti - si >= 0) & (ti - si < window), 1.0, 0.0).astype(bf)
    pos = lax.broadcasted_iota(jnp.int32, (LENGTH, own), 0)
    divisor = jnp.minimum(pos + 1, window).astype(f32)
    for s in range(rows // LENGTH):
        part = normed[s * LENGTH:(s + 1) * LENGTH]
        summed = jnp.dot(band, part, preferred_element_type=f32)
        xn[0, s * LENGTH:(s + 1) * LENGTH, :own] = (summed / divisor - part.astype(f32)).astype(bf)

    def gw_swap(k):
        b = gw_at(zk[k], r)
        got(b, rw.at[k - 1])
        send(b, b, "gwy", ry.at[0], (peer_r, z, t))

    def up_swap(k, parts=whole):
        for i in parts:
            b = up_at(zk[k], r, i)
            got(b, rwu.at[k - 1, i])
            send(b, b, "upy", ryu.at[0], (peer_r, z, t))

    with jax.named_scope("gwswap"):
        for k in (1, 2, 3):
            gw_swap(k)
        up_send(2, outer, early)
        up_send(3, outer, early)
    with jax.named_scope("gwswapped"):
        got(gwg.at[pl.ds(0, (Z - 1) * hg)], ry.at[0])
    with jax.named_scope("mix"):
        mixed = jnp.dot(xn[0, :, :own], gwg[...], preferred_element_type=f32) * gs[...]
        car[z, t] = (tok[:, cols].astype(f32) + mixed).astype(bf)
    H = rows // LENGTH
    hr = LENGTH
    is_in = lax.rem(lax.div(z + 1, 2), 2)
    blocks = (z, is_in * zk[1] + (1 - is_in) * zk[3], is_in * zk[3] + (1 - is_in) * zk[1], zk[2])

    def half(h):
        return pl.ds(h * hr, hr)

    def to_x(src, h):
        b = car.at[src, t, half(h)]
        send(b, b, "carx", rcx.at[src, h], (r, z, xp))

    def to_core(src, h, q):
        b = car.at[src, q, half(h)]
        send(b, b, "carc", rcc.at[src], (r, z, cp))

    def to_z(src, h, dev, when=None):
        b = car.at[src, t, half(h)]
        send(b, b, "carz", rcz.at[src, h], (r, dev, t), when)

    for h in range(H):
        to_z(z, h, zk[3])
        to_z(z, h, mate)
        to_x(z, h)
        to_core(z, h, t)
    up_send(3, inner)
    up_send(2, inner)

    with jax.named_scope("casts"):
        for k in (2, 3, 1):
            loads[("dn", k)].wait()
            for c in range(C):
                dns[k, c] = dnf[k, :, c * cw:(c + 1) * cw].astype(bf)
        loads[("up", 0)].wait()
        upg[pl.ds(pl.multiple_of(z * 2 * hu + r * hu, hu), hu), :] = upf[0].astype(bf)
        loads["upo"].wait()
        upg[pl.ds(pl.multiple_of(z * 2 * hu + peer_r * hu, hu), hu), :] = upo[...].astype(bf)
        loads[("dn", 0)].wait()
        loads["dno"].wait()
        for c in range(C):
            here = pl.ds(mul(z, cw), cw)
            dng[c, pl.ds(mul(r, hd), hd), here] = dnf[0, :, c * cw:(c + 1) * cw].astype(bf)
            dng[c, pl.ds(mul(peer_r, hd), hd), here] = dno[:, c * cw:(c + 1) * cw].astype(bf)

    def arrive(d, h):
        src = blocks[d]
        got(car.at[src, t, half(h)], rcz.at[src, h])
        if d < 3:
            to_z(src, h, mate, outer if d == 1 else inner)
        to_x(src, h)
        to_core(src, h, t)

    def from_x(d, h):
        src = blocks[d]
        got(car.at[src, xp, half(h)], rcx.at[src, h])
        to_core(src, h, xp)

    def dn_group(*pieces):
        for c, k in pieces:
            dn_send(c, k)

    def dn_outer(c):
        dn_group((c, 3), (c, 2), (c, 1))

    def dn_forward(c, k):
        src = zk[k]
        got(dn_at(c, src, r), rwd.at[k - 1, c])
        send(dn_at(c, src, r), dn_at(c, src, r), "dny", ryd.at[c], (peer_r, z, t))

    def norm(d):
        src = blocks[d]
        got(car.at[src, pl.ds(0, 2)], rcc.at[src])
        total = jnp.zeros((rows, 1), f32)
        for q in range(T):
            c = car[src, q].astype(f32)
            total += jnp.sum(c * c, axis=-1, keepdims=True)
        scale = lax.rsqrt(total / D + norm_eps)
        for q in range(T):
            part = slice(q * own, (q + 1) * own)
            xn[d, :, part] = (car[src, q].astype(f32) * scale * lg[:, part]).astype(bf)

    def up(d):
        pre = jnp.dot(xn[d], upg[...], preferred_element_type=f32)
        pre = jnp.maximum(pre * us[:, pl.ds(mul(z, fsub), fsub)], 0.0)
        hid[blocks[d]] = (pre * pre).astype(bf)

    def dn_ready(c):
        got(dns.at[0, pl.ds(0, Z - 1)], ryd.at[c])

    def down(c, k):
        src = zk[k]
        p = jnp.dot(hid[src], dng[c], preferred_element_type=f32)
        for q in range(T):
            part = p[:, q * cw:(q + 1) * cw] * ds[:, q * own + c * cw:q * own + (c + 1) * cw]
            pb[c, src, q] = part.astype(bf)
        for j, q in ((1, cxp), (0, cp)):
            send(pb.at[c, src, q], ra.at[c, src, j], "pb", rx.at[c, src] if j else rj.at[c], (r, z, cp))

    def over_x(c, k):
        src = zk[k]
        got(ra.at[c, src, 1], rx.at[c, src])
        sx[c, src] = (pb[c, src, xp].astype(f32) + ra[c, src, 1].astype(f32)).astype(bf)
        send(sx.at[c, src], rb.at[c, src], "sx", rb_s.at[c, src], (r, z, xp))

    def both(c, src):
        return pb[c, src, t].astype(f32) + ra[c, src, 0].astype(f32) + rb[c, src].astype(f32)

    def joined(c, k):
        src = zk[k]
        if k == 2:
            got(sx.at[c], rj.at[c])
        got(rb.at[c, src], rb_s.at[c, src])

    def to_side(c):
        src = zk[2]
        joined(c, 2)
        sz[c, src] = both(c, src).astype(bf)
        send(sz.at[c, src], ri.at[c], "sz", rm.at[c], (r, mate, t))

    def across(c):
        src = zk[3]
        joined(c, 3)
        got(ri.at[c], rm.at[c])
        sz[c, src] = (both(c, src) + ri[c].astype(f32)).astype(bf)
        send(sz.at[c, src], rc.at[c, 1], "sz", rt.at[c, 1], (r, src, t))

    def to_mate(c):
        joined(c, 1)
        sz[c, mate] = both(c, mate).astype(bf)
        send(sz.at[c, mate], rc.at[c, 0], "sz", rt.at[c, 0], (r, mate, t))

    def write(c, q):
        pltpu.make_async_copy(
            og.at[c, q], out_h.at[:, pl.ds(pl.multiple_of(q * own + c * cw, cw), cw)], sent.at[len(groups)]
        ).start()

    def pass_on(c, q, rs, dev):
        send(og.at[c, q], og.at[c, q], "og", rs, dev)

    def finish(c):
        joined(c, 0)
        acc = both(c, z) + car[z, t, :, :].astype(f32)[:, c * cw:(c + 1) * cw]
        for j in range(2):
            got(rc.at[c, j], rt.at[c, j])
            acc += rc[c, j].astype(f32)
        og[c, t] = acc.astype(bf)
        pass_on(c, t, ro.at[c], (r, z, xp))
        pass_on(c, t, rq.at[c], (r, z, cp))
        write(c, t)

    def spread(c):
        got(og.at[c, xp], ro.at[c])
        pass_on(c, xp, rq.at[c], (r, z, cp))
        write(c, xp)

    def collect(c):
        got(og.at[c, pl.ds(0, 2)], rq.at[c])
        write(c, cp)
        write(c, cxp)

    def up_ready():
        got(ups.at[pl.ds(0, Z - 1)], ryu.at[0])

    def forward(c):
        for k in (1, 2, 3):
            run("fwd", dn_forward, c, k)

    def halves(name, fn, d):
        for h in range(H):
            run(name, fn, d, h)

    only(outer, ("ous3", up_swap, 3, early))
    only(inner, ("ius1", up_swap, 1, early), ("ius2", up_swap, 2, early))
    halves("fx", from_x, 0)
    halves("arr", arrive, 1)
    only(
        outer, ("ou2", up_send, 2, None, late), ("ou3", up_send, 3, None, late), ("ou1", up_send, 1, None, late),
        ("ous1", up_swap, 1), ("ofx", from_x, 1, 0), ("ofx", from_x, 1, 1),
    )
    halves("arr", arrive, 2)
    only(
        inner, ("ifx", from_x, 1, 0), ("ifx", from_x, 1, 1), ("iarr", arrive, 3, 0), ("iarr", arrive, 3, 1),
        ("dn", dn_outer, 0), ("dn", dn_outer, 1),
        ("ius2", up_swap, 2, late), ("ius3", up_swap, 3),
        ("ifx", from_x, 2, 0), ("ifx", from_x, 2, 1),
        ("ius1", up_swap, 1, late), ("dn", dn_outer, 2), ("dn", dn_outer, 3),
    )
    only(
        outer, ("ofx", from_x, 2, 0), ("ofx", from_x, 2, 1), ("oarr", arrive, 3, 0), ("oarr", arrive, 3, 1),
        ("dn", dn_outer, 0), ("dn", dn_outer, 1), ("ous3", up_swap, 3, late), ("ous2", up_swap, 2),
    )
    halves("fx", from_x, 3)
    for d in range(Z):
        run("norm", norm, d)
    run("usd", up_ready)
    forward(0)
    only(outer, ("dn", dn_outer, 2))
    for d in range(Z):
        run("up", up, d)
    forward(1)
    only(outer, ("dn", dn_outer, 3))
    for c in range(C):
        run("ready", dn_ready, c)
        for k in (2, 3, 1, 0):
            run("down", down, c, k)
        if c > 0:
            run("side", to_side, c - 1)
        for k in (2, 3, 1, 0):
            run("x", over_x, c, k)
        if c + 2 < C:
            forward(c + 2)
        if c > 0:
            run("mate", to_mate, c - 1)
            run("across", across, c - 1)
        if c > 1:
            run("fin", finish, c - 2)
    run("side", to_side, C - 1)
    run("mate", to_mate, C - 1)
    run("across", across, C - 1)
    run("fin", finish, C - 2)
    for c in range(C - 2):
        run("spread", spread, c)
    for c in range(C - 2):
        run("coll", collect, c)
    run("spread", spread, C - 2)
    run("fin", finish, C - 1)
    run("coll", collect, C - 2)
    run("spread", spread, C - 1)
    run("coll", collect, C - 1)
    with jax.named_scope("drain"):
        drain()


def fused(mesh_shape, tokens, mix_gain, group_weight, group_scale, mlp_gain, up_weight, up_scale, down_weight, down_scale):
    Z, T = mesh_shape["fs"], mesh_shape["tp"]
    C = CHUNKS
    rows, D = tokens.shape
    own = group_weight.shape[1]
    hg, hu = group_weight.shape[0] // 2, up_weight.shape[0] // 2
    fsub = up_weight.shape[1] // Z
    hd = fsub // 2
    dsub = down_weight.shape[1]
    cw = dsub // C
    bf, f32 = jnp.bfloat16, jnp.float32
    dma = pltpu.SemaphoreType.DMA
    vm = pl.BlockSpec(memory_space=pltpu.VMEM)
    hbm = pl.BlockSpec(memory_space=pl.ANY)
    sizes = (Z, T, C, rows, D, own, hg, hu, hd, fsub, dsub)
    V = pltpu.VMEM
    H = rows // LENGTH
    piece = (C, Z, rows, cw)
    return pl.pallas_call(
        functools.partial(ring_kernel, sizes),
        out_shape=jax.ShapeDtypeStruct((rows, D), bf),
        in_specs=[hbm, vm, hbm, vm, vm, hbm, vm, hbm, vm],
        out_specs=hbm,
        scratch_shapes=[
            V((rows, D), bf), V((2 * hg, own), f32),
            V((Z, hu, fsub), f32), V((hu, fsub), f32), V((Z, hd, dsub), f32), V((hd, dsub), f32),
            V((Z * 2 * hg, own), bf), V((Z, hu, fsub), bf), V((Z * 2 * hu, fsub), bf),
            V((Z, C, hd, cw), bf), V((C, 2 * hd, Z * cw), bf),
            V((Z, T, rows, own), bf), V((Z, rows, D), bf), V((Z, rows, fsub), bf), V((C, Z, T, rows, cw), bf),
            V((C, Z, 2, rows, cw), bf), V(piece, bf), V(piece, bf), V(piece, bf), V((C, rows, cw), bf),
            V((C, 2, rows, cw), bf), V((C, T, rows, cw), bf),
            dma((4 + 2 * Z,)), dma((14,)), dma((3,)), dma((1,)), dma((3, PARTS)), dma((1,)), dma((3, C)), dma((C,)),
            dma((Z, H)), dma((Z, H)), dma((Z,)), dma((C, Z)), dma((C,)), dma((C, Z)), dma((C, 2)), dma((C,)),
            dma((C,)), dma((C,)),
        ],
        compiler_params=pltpu.CompilerParams(
            collective_id=0, has_side_effects=True, vmem_limit_bytes=60 * 1024 * 1024
        ),
    )(
        tokens, mix_gain[None], group_weight, group_scale, mlp_gain[None],
        up_weight, up_scale, down_weight, down_scale,
    )


def fits(mesh):
    shape = mesh.shape
    return shape["rep"] == 2 and shape["tp"] == GROUPS and shape["fs"] == shape["tp"]


def solution(mesh):
    in_specs = (
        P(("rep", "fs"), None),
        P(),
        P("fs", "tp"),
        P(None, "tp"),
        P(),
        P("fs", "tp"),
        P(None, "tp"),
        P("tp", "fs"),
        P(),
    )
    out_specs = P(("rep", "fs"), None)
    chosen = functools.partial(fused, mesh.shape) if fits(mesh) else body
    return jax.shard_map(chosen, mesh=mesh, in_specs=in_specs, out_specs=out_specs, check_vma=False)
```

```python
import functools

import jax
import jax.numpy as jnp
from jax import lax
from jax.experimental import pallas as pl
from jax.experimental.pallas import tpu as pltpu
from jax.sharding import PartitionSpec as P

GROUPS = 4
LENGTH = 128


norm_eps = 1e-06


def norm_rows(values, gain):
    promoted = values.astype(jnp.float32)
    inverse = lax.rsqrt(jnp.mean(promoted * promoted, axis=-1, keepdims=True) + norm_eps)
    return (promoted * inverse * gain).astype(jnp.bfloat16)


def band_means(inputs, window, seq_length):
    row_count, columns = inputs.shape
    by_sequence = inputs.reshape(row_count // seq_length, seq_length, columns)
    position = jnp.arange(seq_length, dtype=jnp.int32)
    offset = position[:, None] - position[None, :]
    band_mask = ((offset >= 0) & (offset < window)).astype(jnp.bfloat16)
    divisor = jnp.minimum(position + 1, window).astype(jnp.float32)
    summed = jnp.einsum("ts,nsc->ntc", band_mask, by_sequence, preferred_element_type=jnp.float32)
    return (summed / divisor[None, :, None] - by_sequence.astype(jnp.float32)).reshape(
        row_count, columns
    )


def body(
    tokens,
    mix_gain,
    group_weight,
    group_scale,
    mlp_gain,
    up_weight,
    up_scale,
    down_weight,
    down_scale,
):
    model_width = tokens.shape[1]
    group_width = model_width // GROUPS
    own_cols = group_weight.shape[1]
    column_start = lax.axis_index("tp") * own_cols
    group_index = column_start // group_width
    normed = norm_rows(tokens, mix_gain)
    inputs = lax.dynamic_slice_in_dim(normed, group_index * group_width, group_width, 1)
    window = jnp.left_shift(jnp.int32(2), group_index)
    pooled = band_means(inputs, window, LENGTH).astype(jnp.bfloat16)
    mixed_cols = (
        jnp.dot(
            pooled,
            lax.all_gather(group_weight.astype(jnp.bfloat16), "fs", axis=0, tiled=True),
            preferred_element_type=jnp.float32,
        )
        * group_scale
    )
    own_tokens = lax.dynamic_slice_in_dim(tokens, column_start, own_cols, 1)
    carried_cols = (own_tokens.astype(jnp.float32) + mixed_cols).astype(jnp.bfloat16)
    carried = lax.all_gather(carried_cols, "tp", axis=1, tiled=True)
    normed_mlp = norm_rows(carried, mlp_gain)
    pre_act = (
        jnp.dot(
            normed_mlp,
            lax.all_gather(up_weight.astype(jnp.bfloat16), "fs", axis=0, tiled=True),
            preferred_element_type=jnp.float32,
        )
        * up_scale
    )
    hidden = jnp.square(jax.nn.relu(pre_act)).astype(jnp.bfloat16)
    partial_value = (
        jnp.dot(
            hidden,
            lax.all_gather(down_weight.astype(jnp.bfloat16), "fs", axis=1, tiled=True),
            preferred_element_type=jnp.float32,
        )
        * down_scale
    )
    summed = lax.psum(partial_value.astype(jnp.bfloat16), "tp").astype(jnp.float32)
    return (carried.astype(jnp.float32) + summed).astype(jnp.bfloat16)


MESH = pl.DeviceIdType.MESH
CHUNKS = 4
PARTS = 4


def ring_kernel(
    sizes,
    tok_h, mg_h, gw_h, gs_h, lg_h, up_h, us_h, dn_h, ds_h,
    out_h,
    mg, gs, lg, us, ds,
    tok, gwf, upf, upo, dnf, dno,
    gwg, ups, upg, dns, dng,
    car, xn, hid, pb, ra, sx, rb, sz, ri, rc,
    ld, sent, rw, ry, rwu, ryu, rwd, ryd, rcz, rcx, rcc, rx, rj, rb_s, rt, rm, ro, rq,
):
    Z, T, C, rows, D, own, hg, hu, hd, fsub, dsub = sizes
    cw = dsub // C
    r, z, t = lax.axis_index("rep"), lax.axis_index("fs"), lax.axis_index("tp")
    cp = t + 1 - 2 * lax.rem(t, 2)
    xp = lax.rem(t + 2, T)
    cxp = lax.rem(cp + 2, T)
    peer_r = 1 - r
    bf, f32 = jnp.bfloat16, jnp.float32
    mate = z + 1 - 2 * lax.rem(z, 2)
    zk = (z, mate, lax.rem(z + 2, Z), Z - 1 - z)
    inner = (z > 0) & (z < Z - 1)
    outer = (z == 0) | (z == Z - 1)

    def mul(i, n):
        return pl.multiple_of(i * n, n)

    loads = {}

    def load(key, src, dst, k):
        c = pltpu.make_async_copy(src, dst, ld.at[k])
        c.start()
        loads[key] = c

    def load_up(k):
        load(("up", k), up_h.at[pl.ds(mul(r, hu), hu), pl.ds(mul(zk[k], fsub), fsub)], upf.at[k], 2 + k)

    def load_dn(k):
        load(("dn", k), dn_h.at[pl.ds(pl.multiple_of(zk[k] * 2 * hd + r * hd, hd), hd), :], dnf.at[k], 2 + Z + k)

    load("gw", gw_h, gwf, 0)
    load_up(2)
    load("tok", tok_h, tok, 1)
    load_up(3)
    load_up(1)
    load_up(0)
    load("upo", up_h.at[pl.ds(mul(peer_r, hu), hu), pl.ds(mul(z, fsub), fsub)], upo, 2 + 2 * Z)
    for k in (2, 3, 1, 0):
        load_dn(k)
    small = (("mg", mg_h, mg), ("gs", gs_h, gs), ("lg", lg_h, lg), ("us", us_h, us), ("ds", ds_h, ds))
    for i, (key, src, dst) in enumerate(small):
        load(key, src, dst, 4 + 2 * Z + i)
    load("dno", dn_h.at[pl.ds(pl.multiple_of(z * 2 * hd + peer_r * hd, hd), hd), :], dno, 3 + 2 * Z)

    barrier = pltpu.get_barrier_semaphore()
    peers = [(r, zk[k], t) for k in range(1, Z)] + [(peer_r, z, t), (r, z, xp), (r, z, cp)]
    for p in peers:
        pl.semaphore_signal(barrier, inc=1, device_id=p, device_id_type=MESH)
    loads["gw"].wait()
    gwg[pl.ds(mul(z, 2 * hg), 2 * hg), :] = gwf[...].astype(bf)
    loads[("up", 2)].wait()
    ups[2] = upf[2].astype(bf)
    with jax.named_scope("barrier"):
        pl.semaphore_wait(barrier, len(peers))

    def remote(src, dst, ss, rs, dev):
        return pltpu.make_async_remote_copy(
            src_ref=src, dst_ref=dst, send_sem=ss, recv_sem=rs, device_id=dev, device_id_type=MESH
        )

    role = [None]

    def guarded(fn, when=None):
        for p in (role[0],):
            if p is not None:
                when = p if when is None else when & p
        if when is None:
            fn()
        else:
            pl.when(when)(fn)
        return when

    groups = ("gw", "gwy", "up", "upy", "dn", "dny", "carz", "carx", "carc", "pb", "sx", "sz", "og")

    def send(src, dst, group, rs, dev, when=None):
        guarded(lambda: remote(src, dst, sent.at[groups.index(group)], rs, dev).start(), when)

    def drain():
        three = pl.ds(1, Z - 1)
        same = (
            gwg.at[pl.ds(0, (Z - 1) * hg)], gwg.at[pl.ds(0, (Z - 1) * hg)], ups.at[three], ups.at[three],
            dns.at[three], dns.at[three], car.at[0, three], car.at[0], car.at[pl.ds(0, 2)],
            ra, rb, sx.at[:, three], sx.at[:, three],
        )
        for i, ref in enumerate(same):
            remote(ref, ref, sent.at[i], rcc.at[0], (peer_r, z, t)).wait_send()

    def got(dst, rs):
        guarded(lambda: remote(dst, dst, sent.at[0], rs, (peer_r, z, t)).wait_recv())

    def only(who, *steps):
        role[0] = who
        for name, fn, *args in steps:
            run(name, fn, *args)
        role[0] = None

    def run(name, fn, *args):
        with jax.named_scope(name + "".join(map(str, [a for a in args if isinstance(a, int)]))):
            fn(*args)

    def gw_at(src, rep):
        return gwg.at[pl.ds(pl.multiple_of(src * 2 * hg + rep * hg, hg), hg), :]

    pu = hu // PARTS

    def up_at(src, rep, i):
        return upg.at[pl.ds(pl.multiple_of(src * 2 * hu + rep * hu + i * pu, pu), pu), :]

    def dn_at(c, src, rep):
        return dng.at[c, pl.ds(mul(rep, hd), hd), pl.ds(mul(src, cw), cw)]

    early, late = range(PARTS // 2), range(PARTS // 2, PARTS)
    whole = range(PARTS)

    def up_send(k, when=None, parts=whole):
        for i in parts:
            piece = ups.at[k, pl.ds(i * pu, pu)]
            send(piece, up_at(z, r, i), "up", rwu.at[k - 1, i], (r, zk[k], t), when)

    def dn_send(c, k):
        send(dns.at[k, c], dn_at(c, z, r), "dn", rwd.at[k - 1, c], (r, zk[k], t))

    for k in (3, 2, 1):
        send(gw_at(z, r), gw_at(z, r), "gw", rw.at[k - 1], (r, zk[k], t))
    loads[("up", 1)].wait()
    ups[1] = upf[1].astype(bf)
    loads[("up", 3)].wait()
    ups[3] = upf[3].astype(bf)
    up_send(1, None, early)
    up_send(1, inner, late)

    for key in ("tok", "mg", "gs", "lg", "us", "ds"):
        loads[key].wait()
    full = tok[...].astype(f32)
    inv = lax.rsqrt(jnp.mean(full * full, axis=-1, keepdims=True) + norm_eps)
    cols = pl.ds(mul(t, own), own)
    mine = tok[:, cols].astype(f32)
    normed = (mine * inv * mg[:, cols]).astype(bf)
    window = jnp.left_shift(jnp.int32(2), t)
    ti = lax.broadcasted_iota(jnp.int32, (LENGTH, LENGTH), 0)
    si = lax.broadcasted_iota(jnp.int32, (LENGTH, LENGTH), 1)
    band = jnp.where((ti - si >= 0) & (ti - si < window), 1.0, 0.0).astype(bf)
    pos = lax.broadcasted_iota(jnp.int32, (LENGTH, own), 0)
    divisor = jnp.minimum(pos + 1, window).astype(f32)
    for s in range(rows // LENGTH):
        part = normed[s * LENGTH:(s + 1) * LENGTH]
        summed = jnp.dot(band, part, preferred_element_type=f32)
        xn[0, s * LENGTH:(s + 1) * LENGTH, :own] = (summed / divisor - part.astype(f32)).astype(bf)

    def gw_swap(k):
        b = gw_at(zk[k], r)
        got(b, rw.at[k - 1])
        send(b, b, "gwy", ry.at[0], (peer_r, z, t))

    def up_swap(k, parts=whole):
        for i in parts:
            b = up_at(zk[k], r, i)
            got(b, rwu.at[k - 1, i])
            send(b, b, "upy", ryu.at[0], (peer_r, z, t))

    with jax.named_scope("gwswap"):
        for k in (1, 2, 3):
            gw_swap(k)
        up_send(2, outer, early)
        up_send(3, outer, early)
    with jax.named_scope("gwswapped"):
        got(gwg.at[pl.ds(0, (Z - 1) * hg)], ry.at[0])
    with jax.named_scope("mix"):
        mixed = jnp.dot(xn[0, :, :own], gwg[...], preferred_element_type=f32) * gs[...]
        car[z, t] = (tok[:, cols].astype(f32) + mixed).astype(bf)
    H = rows // LENGTH
    hr = LENGTH
    is_in = lax.rem(lax.div(z + 1, 2), 2)
    blocks = (z, is_in * zk[1] + (1 - is_in) * zk[3], is_in * zk[3] + (1 - is_in) * zk[1], zk[2])

    def half(h):
        return pl.ds(h * hr, hr)

    def to_x(src, h):
        b = car.at[src, t, half(h)]
        send(b, b, "carx", rcx.at[src, h], (r, z, xp))

    def to_core(src, h, q):
        b = car.at[src, q, half(h)]
        send(b, b, "carc", rcc.at[src], (r, z, cp))

    def to_z(src, h, dev, when=None):
        b = car.at[src, t, half(h)]
        send(b, b, "carz", rcz.at[src, h], (r, dev, t), when)

    for h in range(H):
        to_z(z, h, zk[3])
        to_z(z, h, mate)
        to_x(z, h)
        to_core(z, h, t)
    up_send(2, inner)
    up_send(3, inner)

    with jax.named_scope("casts"):
        for k in (2, 3, 1):
            loads[("dn", k)].wait()
            for c in range(C):
                dns[k, c] = dnf[k, :, c * cw:(c + 1) * cw].astype(bf)
        loads[("up", 0)].wait()
        upg[pl.ds(pl.multiple_of(z * 2 * hu + r * hu, hu), hu), :] = upf[0].astype(bf)
        loads["upo"].wait()
        upg[pl.ds(pl.multiple_of(z * 2 * hu + peer_r * hu, hu), hu), :] = upo[...].astype(bf)
        loads[("dn", 0)].wait()
        loads["dno"].wait()
        for c in range(C):
            here = pl.ds(mul(z, cw), cw)
            dng[c, pl.ds(mul(r, hd), hd), here] = dnf[0, :, c * cw:(c + 1) * cw].astype(bf)
            dng[c, pl.ds(mul(peer_r, hd), hd), here] = dno[:, c * cw:(c + 1) * cw].astype(bf)

    def arrive(d, h):
        src = blocks[d]
        got(car.at[src, t, half(h)], rcz.at[src, h])
        if d < 3:
            to_z(src, h, mate, outer if d == 1 else inner)
        to_x(src, h)
        to_core(src, h, t)

    def from_x(d, h):
        src = blocks[d]
        got(car.at[src, xp, half(h)], rcx.at[src, h])
        to_core(src, h, xp)

    def dn_group(*pieces):
        for c, k in pieces:
            dn_send(c, k)

    def dn_outer(c):
        dn_group((c, 3), (c, 2), (c, 1))

    def dn_forward(c, k):
        src = zk[k]
        got(dn_at(c, src, r), rwd.at[k - 1, c])
        send(dn_at(c, src, r), dn_at(c, src, r), "dny", ryd.at[c], (peer_r, z, t))

    def norm(d):
        src = blocks[d]
        got(car.at[src, pl.ds(0, 2)], rcc.at[src])
        total = jnp.zeros((rows, 1), f32)
        for q in range(T):
            c = car[src, q].astype(f32)
            total += jnp.sum(c * c, axis=-1, keepdims=True)
        scale = lax.rsqrt(total / D + norm_eps)
        for q in range(T):
            part = slice(q * own, (q + 1) * own)
            xn[d, :, part] = (car[src, q].astype(f32) * scale * lg[:, part]).astype(bf)

    def up(d):
        pre = jnp.dot(xn[d], upg[...], preferred_element_type=f32)
        pre = jnp.maximum(pre * us[:, pl.ds(mul(z, fsub), fsub)], 0.0)
        hid[blocks[d]] = (pre * pre).astype(bf)

    def dn_ready(c):
        got(dns.at[0, pl.ds(0, Z - 1)], ryd.at[c])

    def down(c, k):
        src = zk[k]
        p = jnp.dot(hid[src], dng[c], preferred_element_type=f32)
        for q in range(T):
            part = p[:, q * cw:(q + 1) * cw] * ds[:, q * own + c * cw:q * own + (c + 1) * cw]
            pb[c, src, q] = part.astype(bf)
        for j, q in ((1, cxp), (0, cp)):
            send(pb.at[c, src, q], ra.at[c, src, j], "pb", rx.at[c, src] if j else rj.at[c], (r, z, cp))

    def over_x(c, k):
        src = zk[k]
        got(ra.at[c, src, 1], rx.at[c, src])
        sx[c, src] = (pb[c, src, xp].astype(f32) + ra[c, src, 1].astype(f32)).astype(bf)
        send(sx.at[c, src], rb.at[c, src], "sx", rb_s.at[c, src], (r, z, xp))

    def both(c, src):
        return pb[c, src, t].astype(f32) + ra[c, src, 0].astype(f32) + rb[c, src].astype(f32)

    def joined(c, k):
        src = zk[k]
        if k == 2:
            got(sx.at[c], rj.at[c])
        got(rb.at[c, src], rb_s.at[c, src])

    def to_side(c):
        src = zk[2]
        joined(c, 2)
        sz[c, src] = both(c, src).astype(bf)
        send(sz.at[c, src], ri.at[c], "sz", rm.at[c], (r, mate, t))

    def across(c):
        src = zk[3]
        joined(c, 3)
        got(ri.at[c], rm.at[c])
        sz[c, src] = (both(c, src) + ri[c].astype(f32)).astype(bf)
        send(sz.at[c, src], rc.at[c, 1], "sz", rt.at[c, 1], (r, src, t))

    def to_mate(c):
        joined(c, 1)
        sz[c, mate] = both(c, mate).astype(bf)
        send(sz.at[c, mate], rc.at[c, 0], "sz", rt.at[c, 0], (r, mate, t))

    def og(c, q):
        return out_h.at[:, pl.ds(pl.multiple_of(q * own + c * cw, cw), cw)]

    def pass_on(c, q, rs, dev):
        send(og(c, q), og(c, q), "og", rs, dev)

    def finish(c):
        joined(c, 0)
        acc = both(c, z) + car[z, t, :, :].astype(f32)[:, c * cw:(c + 1) * cw]
        for j in range(2):
            got(rc.at[c, j], rt.at[c, j])
            acc += rc[c, j].astype(f32)
        out_h[:, pl.ds(pl.multiple_of(t * own + c * cw, cw), cw)] = acc.astype(bf)
        pass_on(c, t, ro.at[c], (r, z, xp))
        pass_on(c, t, rq.at[c], (r, z, cp))

    def spread(c):
        got(og(c, xp), ro.at[c])
        pass_on(c, xp, rq.at[c], (r, z, cp))

    def collect(c):
        got(sx.at[c, pl.ds(0, 2)], rq.at[c])

    def up_ready():
        got(ups.at[pl.ds(0, Z - 1)], ryu.at[0])

    def forward(c):
        for k in (1, 2, 3):
            run("fwd", dn_forward, c, k)

    def halves(name, fn, d):
        for h in range(H):
            run(name, fn, d, h)

    only(outer, ("ous3", up_swap, 3, early))
    only(inner, ("ius1", up_swap, 1, early), ("ius2", up_swap, 2, early))
    halves("fx", from_x, 0)
    halves("arr", arrive, 1)
    only(
        outer, ("ou2", up_send, 2, None, late), ("ou3", up_send, 3, None, late), ("ou1", up_send, 1, None, late),
        ("ous1", up_swap, 1), ("ofx", from_x, 1, 0), ("ofx", from_x, 1, 1),
    )
    halves("arr", arrive, 2)
    only(
        inner, ("ifx", from_x, 1, 0), ("ifx", from_x, 1, 1), ("iarr", arrive, 3, 0), ("iarr", arrive, 3, 1),
        ("dn", dn_outer, 0), ("dn", dn_outer, 1),
        ("ius2", up_swap, 2, late), ("ius3", up_swap, 3),
        ("ifx", from_x, 2, 0), ("ifx", from_x, 2, 1),
        ("ius1", up_swap, 1, late), ("dn", dn_outer, 2), ("dn", dn_outer, 3),
    )
    only(
        outer, ("ofx", from_x, 2, 0), ("ofx", from_x, 2, 1), ("oarr", arrive, 3, 0), ("oarr", arrive, 3, 1),
        ("ous3", up_swap, 3, late), ("ous2", up_swap, 2), ("dn", dn_outer, 0),
    )
    halves("fx", from_x, 3)
    for d in range(Z):
        run("norm", norm, d)
    run("usd", up_ready)
    only(outer, ("dn", dn_outer, 1))
    forward(0)
    only(outer, ("dn", dn_outer, 2))
    for d in range(Z):
        run("up", up, d)
    forward(1)
    only(outer, ("dn", dn_outer, 3))
    for c in range(C):
        run("ready", dn_ready, c)
        for k in (2, 3, 1, 0):
            run("down", down, c, k)
        if c > 0:
            run("side", to_side, c - 1)
        for k in (2, 3, 1, 0):
            run("x", over_x, c, k)
        if c + 2 < C:
            forward(c + 2)
        if c > 0:
            run("mate", to_mate, c - 1)
            run("across", across, c - 1)
        if c > 1:
            run("fin", finish, c - 2)
    run("side", to_side, C - 1)
    run("mate", to_mate, C - 1)
    run("across", across, C - 1)
    run("fin", finish, C - 2)
    for c in range(C - 2):
        run("spread", spread, c)
    for c in range(C - 2):
        run("coll", collect, c)
    run("spread", spread, C - 2)
    run("fin", finish, C - 1)
    run("coll", collect, C - 2)
    run("spread", spread, C - 1)
    run("coll", collect, C - 1)
    with jax.named_scope("drain"):
        drain()


def fused(mesh_shape, tokens, mix_gain, group_weight, group_scale, mlp_gain, up_weight, up_scale, down_weight, down_scale):
    Z, T = mesh_shape["fs"], mesh_shape["tp"]
    C = CHUNKS
    rows, D = tokens.shape
    own = group_weight.shape[1]
    hg, hu = group_weight.shape[0] // 2, up_weight.shape[0] // 2
    fsub = up_weight.shape[1] // Z
    hd = fsub // 2
    dsub = down_weight.shape[1]
    cw = dsub // C
    bf, f32 = jnp.bfloat16, jnp.float32
    dma = pltpu.SemaphoreType.DMA
    vm = pl.BlockSpec(memory_space=pltpu.VMEM)
    hbm = pl.BlockSpec(memory_space=pltpu.HBM)
    sizes = (Z, T, C, rows, D, own, hg, hu, hd, fsub, dsub)
    V = pltpu.VMEM
    H = rows // LENGTH
    piece = (C, Z, rows, cw)
    pin = functools.partial(pltpu.with_memory_space_constraint, memory_space=pltpu.HBM)
    return pl.pallas_call(
        functools.partial(ring_kernel, sizes),
        out_shape=jax.ShapeDtypeStruct((rows, D), bf),
        in_specs=[hbm] * 9,
        out_specs=vm,
        scratch_shapes=[
            V((1, D), f32), V((1, own), f32), V((1, D), f32), V((1, Z * fsub), f32), V((1, D), f32),
            V((rows, D), bf), V((2 * hg, own), f32),
            V((Z, hu, fsub), f32), V((hu, fsub), f32), V((Z, hd, dsub), f32), V((hd, dsub), f32),
            V((Z * 2 * hg, own), bf), V((Z, hu, fsub), bf), V((Z * 2 * hu, fsub), bf),
            V((Z, C, hd, cw), bf), V((C, 2 * hd, Z * cw), bf),
            V((Z, T, rows, own), bf), V((Z, rows, D), bf), V((Z, rows, fsub), bf), V((C, Z, T, rows, cw), bf),
            V((C, Z, 2, rows, cw), bf), V(piece, bf), V(piece, bf), V(piece, bf), V((C, rows, cw), bf),
            V((C, 2, rows, cw), bf),
            dma((9 + 2 * Z,)), dma((13,)), dma((3,)), dma((1,)), dma((3, PARTS)), dma((1,)), dma((3, C)), dma((C,)),
            dma((Z, H)), dma((Z, H)), dma((Z,)), dma((C, Z)), dma((C,)), dma((C, Z)), dma((C, 2)), dma((C,)),
            dma((C,)), dma((C,)),
        ],
        compiler_params=pltpu.CompilerParams(
            collective_id=0, has_side_effects=True, vmem_limit_bytes=48000 * 1024
        ),
    )(
        *(pin(a) for a in (
            tokens, mix_gain[None], group_weight, group_scale, mlp_gain[None],
            up_weight, up_scale, down_weight, down_scale,
        ))
    )


def fits(mesh):
    shape = mesh.shape
    return shape["rep"] == 2 and shape["tp"] == GROUPS and shape["fs"] == shape["tp"]


def solution(mesh):
    in_specs = (
        P(("rep", "fs"), None),
        P(),
        P("fs", "tp"),
        P(None, "tp"),
        P(),
        P("fs", "tp"),
        P(None, "tp"),
        P("tp", "fs"),
        P(),
    )
    out_specs = P(("rep", "fs"), None)
    chosen = functools.partial(fused, mesh.shape) if fits(mesh) else body
    return jax.shard_map(chosen, mesh=mesh, in_specs=in_specs, out_specs=out_specs, check_vma=False)
```

```python
import functools

import jax
import jax.numpy as jnp
from jax import lax
from jax.experimental import pallas as pl
from jax.experimental.pallas import tpu as pltpu
from jax.sharding import PartitionSpec as P

GROUPS = 4
LENGTH = 128


norm_eps = 1e-06


def norm_rows(values, gain):
    promoted = values.astype(jnp.float32)
    inverse = lax.rsqrt(jnp.mean(promoted * promoted, axis=-1, keepdims=True) + norm_eps)
    return (promoted * inverse * gain).astype(jnp.bfloat16)


def band_means(inputs, window, seq_length):
    row_count, columns = inputs.shape
    by_sequence = inputs.reshape(row_count // seq_length, seq_length, columns)
    position = jnp.arange(seq_length, dtype=jnp.int32)
    offset = position[:, None] - position[None, :]
    band_mask = ((offset >= 0) & (offset < window)).astype(jnp.bfloat16)
    divisor = jnp.minimum(position + 1, window).astype(jnp.float32)
    summed = jnp.einsum("ts,nsc->ntc", band_mask, by_sequence, preferred_element_type=jnp.float32)
    return (summed / divisor[None, :, None] - by_sequence.astype(jnp.float32)).reshape(
        row_count, columns
    )


def body(
    tokens,
    mix_gain,
    group_weight,
    group_scale,
    mlp_gain,
    up_weight,
    up_scale,
    down_weight,
    down_scale,
):
    model_width = tokens.shape[1]
    group_width = model_width // GROUPS
    own_cols = group_weight.shape[1]
    column_start = lax.axis_index("tp") * own_cols
    group_index = column_start // group_width
    normed = norm_rows(tokens, mix_gain)
    inputs = lax.dynamic_slice_in_dim(normed, group_index * group_width, group_width, 1)
    window = jnp.left_shift(jnp.int32(2), group_index)
    pooled = band_means(inputs, window, LENGTH).astype(jnp.bfloat16)
    mixed_cols = (
        jnp.dot(
            pooled,
            lax.all_gather(group_weight.astype(jnp.bfloat16), "fs", axis=0, tiled=True),
            preferred_element_type=jnp.float32,
        )
        * group_scale
    )
    own_tokens = lax.dynamic_slice_in_dim(tokens, column_start, own_cols, 1)
    carried_cols = (own_tokens.astype(jnp.float32) + mixed_cols).astype(jnp.bfloat16)
    carried = lax.all_gather(carried_cols, "tp", axis=1, tiled=True)
    normed_mlp = norm_rows(carried, mlp_gain)
    pre_act = (
        jnp.dot(
            normed_mlp,
            lax.all_gather(up_weight.astype(jnp.bfloat16), "fs", axis=0, tiled=True),
            preferred_element_type=jnp.float32,
        )
        * up_scale
    )
    hidden = jnp.square(jax.nn.relu(pre_act)).astype(jnp.bfloat16)
    partial_value = (
        jnp.dot(
            hidden,
            lax.all_gather(down_weight.astype(jnp.bfloat16), "fs", axis=1, tiled=True),
            preferred_element_type=jnp.float32,
        )
        * down_scale
    )
    summed = lax.psum(partial_value.astype(jnp.bfloat16), "tp").astype(jnp.float32)
    return (carried.astype(jnp.float32) + summed).astype(jnp.bfloat16)


MESH = pl.DeviceIdType.MESH
CHUNKS = 4
PARTS = 4


def ring_kernel(
    sizes,
    tok_h, mg_h, gw_h, gs_h, lg_h, up_h, us_h, dn_h, ds_h,
    out_h,
    mg, gs, lg, us, ds,
    tok, gwf, upf, upo, dnf, dno,
    gwg, ups, upg, dns, dng,
    car, xn, hid, pb, ra, sx, rb, sz, ri, rc,
    ld, sent, rw, ry, rwu, ryu, rwd, ryd, rcz, rcx, rcc, rx, rj, rb_s, rt, rm, ro, rq,
):
    Z, T, C, rows, D, own, hg, hu, hd, fsub, dsub = sizes
    cw = dsub // C
    r, z, t = lax.axis_index("rep"), lax.axis_index("fs"), lax.axis_index("tp")
    cp = t + 1 - 2 * lax.rem(t, 2)
    xp = lax.rem(t + 2, T)
    cxp = lax.rem(cp + 2, T)
    peer_r = 1 - r
    bf, f32 = jnp.bfloat16, jnp.float32
    mate = z + 1 - 2 * lax.rem(z, 2)
    zk = (z, mate, lax.rem(z + 2, Z), Z - 1 - z)
    inner = (z > 0) & (z < Z - 1)
    outer = (z == 0) | (z == Z - 1)

    def mul(i, n):
        return pl.multiple_of(i * n, n)

    loads = {}

    def load(key, src, dst, k):
        c = pltpu.make_async_copy(src, dst, ld.at[k])
        c.start()
        loads[key] = c

    def load_up(k):
        load(("up", k), up_h.at[pl.ds(mul(r, hu), hu), pl.ds(mul(zk[k], fsub), fsub)], upf.at[k], 2 + k)

    def load_dn(k):
        load(("dn", k), dn_h.at[pl.ds(pl.multiple_of(zk[k] * 2 * hd + r * hd, hd), hd), :], dnf.at[k], 2 + Z + k)

    load("gw", gw_h, gwf, 0)
    load_up(2)
    load("tok", tok_h, tok, 1)
    load_up(3)
    load_up(1)
    load_up(0)
    load("upo", up_h.at[pl.ds(mul(peer_r, hu), hu), pl.ds(mul(z, fsub), fsub)], upo, 2 + 2 * Z)
    for k in (2, 3, 1, 0):
        load_dn(k)
    small = (("mg", mg_h, mg), ("gs", gs_h, gs), ("lg", lg_h, lg), ("us", us_h, us), ("ds", ds_h, ds))
    for i, (key, src, dst) in enumerate(small):
        load(key, src, dst, 4 + 2 * Z + i)
    load("dno", dn_h.at[pl.ds(pl.multiple_of(z * 2 * hd + peer_r * hd, hd), hd), :], dno, 3 + 2 * Z)

    barrier = pltpu.get_barrier_semaphore()
    peers = [(r, zk[k], t) for k in range(1, Z)] + [(peer_r, z, t), (r, z, xp), (r, z, cp)]
    for p in peers:
        pl.semaphore_signal(barrier, inc=1, device_id=p, device_id_type=MESH)
    loads["gw"].wait()
    gwg[pl.ds(mul(z, 2 * hg), 2 * hg), :] = gwf[...].astype(bf)
    loads[("up", 2)].wait()
    ups[2] = upf[2].astype(bf)
    with jax.named_scope("barrier"):
        pl.semaphore_wait(barrier, len(peers))

    def remote(src, dst, ss, rs, dev):
        return pltpu.make_async_remote_copy(
            src_ref=src, dst_ref=dst, send_sem=ss, recv_sem=rs, device_id=dev, device_id_type=MESH
        )

    role = [None]

    def guarded(fn, when=None):
        for p in (role[0],):
            if p is not None:
                when = p if when is None else when & p
        if when is None:
            fn()
        else:
            pl.when(when)(fn)
        return when

    groups = ("gw", "gwy", "up", "upy", "dn", "dny", "carz", "carx", "carc", "pb", "sx", "sz", "og")

    def send(src, dst, group, rs, dev, when=None):
        guarded(lambda: remote(src, dst, sent.at[groups.index(group)], rs, dev).start(), when)

    def drain():
        three = pl.ds(1, Z - 1)
        same = (
            gwg.at[pl.ds(0, (Z - 1) * hg)], gwg.at[pl.ds(0, (Z - 1) * hg)], ups.at[three], ups.at[three],
            dns.at[three], dns.at[three], car.at[0, three], car.at[0], car.at[pl.ds(0, 2)],
            ra, rb, sx.at[:, three], sx.at[:, three],
        )
        for i, ref in enumerate(same):
            remote(ref, ref, sent.at[i], rcc.at[0], (peer_r, z, t)).wait_send()

    def got(dst, rs):
        guarded(lambda: remote(dst, dst, sent.at[0], rs, (peer_r, z, t)).wait_recv())

    def only(who, *steps):
        role[0] = who
        for name, fn, *args in steps:
            run(name, fn, *args)
        role[0] = None

    def run(name, fn, *args):
        with jax.named_scope(name + "".join(map(str, [a for a in args if isinstance(a, int)]))):
            fn(*args)

    def gw_at(src, rep):
        return gwg.at[pl.ds(pl.multiple_of(src * 2 * hg + rep * hg, hg), hg), :]

    pu = hu // PARTS

    def up_at(src, rep, i):
        return upg.at[pl.ds(pl.multiple_of(src * 2 * hu + rep * hu + i * pu, pu), pu), :]

    def dn_at(c, src, rep):
        return dng.at[c, pl.ds(mul(rep, hd), hd), pl.ds(mul(src, cw), cw)]

    early, late = range(PARTS // 2), range(PARTS // 2, PARTS)
    whole = range(PARTS)

    def up_send(k, when=None, parts=whole):
        for i in parts:
            piece = ups.at[k, pl.ds(i * pu, pu)]
            send(piece, up_at(z, r, i), "up", rwu.at[k - 1, i], (r, zk[k], t), when)

    def dn_send(c, k):
        send(dns.at[k, c], dn_at(c, z, r), "dn", rwd.at[k - 1, c], (r, zk[k], t))

    for k in (3, 2, 1):
        send(gw_at(z, r), gw_at(z, r), "gw", rw.at[k - 1], (r, zk[k], t))
    loads[("up", 1)].wait()
    ups[1] = upf[1].astype(bf)
    loads[("up", 3)].wait()
    ups[3] = upf[3].astype(bf)
    up_send(1, None, early)
    up_send(1, inner, late)

    for key in ("tok", "mg", "gs", "lg", "us", "ds"):
        loads[key].wait()
    full = tok[...].astype(f32)
    inv = lax.rsqrt(jnp.mean(full * full, axis=-1, keepdims=True) + norm_eps)
    cols = pl.ds(mul(t, own), own)
    mine = tok[:, cols].astype(f32)
    normed = (mine * inv * mg[:, cols]).astype(bf)
    window = jnp.left_shift(jnp.int32(2), t)
    ti = lax.broadcasted_iota(jnp.int32, (LENGTH, LENGTH), 0)
    si = lax.broadcasted_iota(jnp.int32, (LENGTH, LENGTH), 1)
    band = jnp.where((ti - si >= 0) & (ti - si < window), 1.0, 0.0).astype(bf)
    pos = lax.broadcasted_iota(jnp.int32, (LENGTH, own), 0)
    divisor = jnp.minimum(pos + 1, window).astype(f32)
    for s in range(rows // LENGTH):
        part = normed[s * LENGTH:(s + 1) * LENGTH]
        summed = jnp.dot(band, part, preferred_element_type=f32)
        xn[0, s * LENGTH:(s + 1) * LENGTH, :own] = (summed / divisor - part.astype(f32)).astype(bf)

    def gw_swap(k):
        b = gw_at(zk[k], r)
        got(b, rw.at[k - 1])
        send(b, b, "gwy", ry.at[0], (peer_r, z, t))

    def up_swap(k, parts=whole):
        for i in parts:
            b = up_at(zk[k], r, i)
            got(b, rwu.at[k - 1, i])
            send(b, b, "upy", ryu.at[0], (peer_r, z, t))

    up_send(2, inner, early)
    with jax.named_scope("gwswap"):
        for k in (1, 2, 3):
            gw_swap(k)
        up_send(2, outer, early)
        up_send(3, outer, early)
    with jax.named_scope("gwswapped"):
        got(gwg.at[pl.ds(0, (Z - 1) * hg)], ry.at[0])
    with jax.named_scope("mix"):
        mixed = jnp.dot(xn[0, :, :own], gwg[...], preferred_element_type=f32) * gs[...]
        car[z, t] = (tok[:, cols].astype(f32) + mixed).astype(bf)
    H = rows // LENGTH
    hr = LENGTH
    is_in = lax.rem(lax.div(z + 1, 2), 2)
    blocks = (z, is_in * zk[1] + (1 - is_in) * zk[3], is_in * zk[3] + (1 - is_in) * zk[1], zk[2])

    def half(h):
        return pl.ds(h * hr, hr)

    def to_x(src, h):
        b = car.at[src, t, half(h)]
        send(b, b, "carx", rcx.at[src, h], (r, z, xp))

    def to_core(src, h, q):
        b = car.at[src, q, half(h)]
        send(b, b, "carc", rcc.at[src], (r, z, cp))

    def to_z(src, h, dev, when=None):
        b = car.at[src, t, half(h)]
        send(b, b, "carz", rcz.at[src, h], (r, dev, t), when)

    for h in range(H):
        to_z(z, h, zk[3])
        to_z(z, h, mate)
        to_x(z, h)
        to_core(z, h, t)
    up_send(3, inner, early)
    for parts in (late,):
        up_send(2, inner, parts)
        up_send(3, inner, parts)

    with jax.named_scope("casts"):
        for k in (2, 3, 1):
            loads[("dn", k)].wait()
            for c in range(C):
                dns[k, c] = dnf[k, :, c * cw:(c + 1) * cw].astype(bf)
        loads[("up", 0)].wait()
        upg[pl.ds(pl.multiple_of(z * 2 * hu + r * hu, hu), hu), :] = upf[0].astype(bf)
        loads["upo"].wait()
        upg[pl.ds(pl.multiple_of(z * 2 * hu + peer_r * hu, hu), hu), :] = upo[...].astype(bf)
        loads[("dn", 0)].wait()
        loads["dno"].wait()
        for c in range(C):
            here = pl.ds(mul(z, cw), cw)
            dng[c, pl.ds(mul(r, hd), hd), here] = dnf[0, :, c * cw:(c + 1) * cw].astype(bf)
            dng[c, pl.ds(mul(peer_r, hd), hd), here] = dno[:, c * cw:(c + 1) * cw].astype(bf)

    def arrive(d, h):
        src = blocks[d]
        got(car.at[src, t, half(h)], rcz.at[src, h])
        if d < 3:
            to_z(src, h, mate, outer if d == 1 else inner)
        to_x(src, h)
        to_core(src, h, t)

    def from_x(d, h):
        src = blocks[d]
        got(car.at[src, xp, half(h)], rcx.at[src, h])
        to_core(src, h, xp)

    def dn_group(*pieces):
        for c, k in pieces:
            dn_send(c, k)

    def dn_outer(c):
        dn_group((c, 3), (c, 2), (c, 1))

    def dn_forward(c, k):
        src = zk[k]
        got(dn_at(c, src, r), rwd.at[k - 1, c])
        send(dn_at(c, src, r), dn_at(c, src, r), "dny", ryd.at[c], (peer_r, z, t))

    def norm(d):
        src = blocks[d]
        got(car.at[src, pl.ds(0, 2)], rcc.at[src])
        total = jnp.zeros((rows, 1), f32)
        for q in range(T):
            c = car[src, q].astype(f32)
            total += jnp.sum(c * c, axis=-1, keepdims=True)
        scale = lax.rsqrt(total / D + norm_eps)
        for q in range(T):
            part = slice(q * own, (q + 1) * own)
            xn[d, :, part] = (car[src, q].astype(f32) * scale * lg[:, part]).astype(bf)

    def up(d):
        pre = jnp.dot(xn[d], upg[...], preferred_element_type=f32)
        pre = jnp.maximum(pre * us[:, pl.ds(mul(z, fsub), fsub)], 0.0)
        hid[blocks[d]] = (pre * pre).astype(bf)

    def dn_ready(c):
        got(dns.at[0, pl.ds(0, Z - 1)], ryd.at[c])

    def down(c, k):
        src = zk[k]
        p = jnp.dot(hid[src], dng[c], preferred_element_type=f32)
        for q in range(T):
            part = p[:, q * cw:(q + 1) * cw] * ds[:, q * own + c * cw:q * own + (c + 1) * cw]
            pb[c, src, q] = part.astype(bf)
        for j, q in ((1, cxp), (0, cp)):
            send(pb.at[c, src, q], ra.at[c, src, j], "pb", rx.at[c, src] if j else rj.at[c], (r, z, cp))

    def over_x(c, k):
        src = zk[k]
        got(ra.at[c, src, 1], rx.at[c, src])
        sx[c, src] = (pb[c, src, xp].astype(f32) + ra[c, src, 1].astype(f32)).astype(bf)
        send(sx.at[c, src], rb.at[c, src], "sx", rb_s.at[c, src], (r, z, xp))

    def both(c, src):
        return pb[c, src, t].astype(f32) + ra[c, src, 0].astype(f32) + rb[c, src].astype(f32)

    def joined(c, k):
        src = zk[k]
        if k == 2:
            got(sx.at[c], rj.at[c])
        got(rb.at[c, src], rb_s.at[c, src])

    def to_side(c):
        src = zk[2]
        joined(c, 2)
        sz[c, src] = both(c, src).astype(bf)
        send(sz.at[c, src], ri.at[c], "sz", rm.at[c], (r, mate, t))

    def across(c):
        src = zk[3]
        joined(c, 3)
        got(ri.at[c], rm.at[c])
        sz[c, src] = (both(c, src) + ri[c].astype(f32)).astype(bf)
        send(sz.at[c, src], rc.at[c, 1], "sz", rt.at[c, 1], (r, src, t))

    def to_mate(c):
        joined(c, 1)
        sz[c, mate] = both(c, mate).astype(bf)
        send(sz.at[c, mate], rc.at[c, 0], "sz", rt.at[c, 0], (r, mate, t))

    def og(c, q):
        return out_h.at[:, pl.ds(pl.multiple_of(q * own + c * cw, cw), cw)]

    def pass_on(c, q, rs, dev):
        send(og(c, q), og(c, q), "og", rs, dev)

    def finish(c):
        joined(c, 0)
        acc = both(c, z) + car[z, t, :, :].astype(f32)[:, c * cw:(c + 1) * cw]
        for j in range(2):
            got(rc.at[c, j], rt.at[c, j])
            acc += rc[c, j].astype(f32)
        out_h[:, pl.ds(pl.multiple_of(t * own + c * cw, cw), cw)] = acc.astype(bf)
        pass_on(c, t, ro.at[c], (r, z, xp))
        pass_on(c, t, rq.at[c], (r, z, cp))

    def spread(c):
        got(og(c, xp), ro.at[c])
        pass_on(c, xp, rq.at[c], (r, z, cp))

    def collect(c):
        got(sx.at[c, pl.ds(0, 2)], rq.at[c])

    def up_ready():
        got(ups.at[pl.ds(0, Z - 1)], ryu.at[0])

    def forward(c):
        for k in (1, 2, 3):
            run("fwd", dn_forward, c, k)

    def halves(name, fn, d):
        for h in range(H):
            run(name, fn, d, h)

    only(outer, ("ous3", up_swap, 3, early))
    only(inner, ("ius1", up_swap, 1, early), ("ius2", up_swap, 2, early))
    halves("fx", from_x, 0)
    halves("arr", arrive, 1)
    only(
        outer, ("ou2", up_send, 2, None, late), ("ou3", up_send, 3, None, late), ("ou1", up_send, 1, None, late),
        ("ous1", up_swap, 1), ("ofx", from_x, 1, 0), ("ofx", from_x, 1, 1),
    )
    halves("arr", arrive, 2)
    only(
        inner, ("ifx", from_x, 1, 0), ("ifx", from_x, 1, 1), ("iarr", arrive, 3, 0), ("iarr", arrive, 3, 1),
        ("dn", dn_outer, 0), ("dn", dn_outer, 1),
        ("ius2", up_swap, 2, late), ("ius1", up_swap, 1, late),
        ("ifx", from_x, 2, 0), ("ifx", from_x, 2, 1),
        ("ius3", up_swap, 3), ("dn", dn_outer, 2), ("dn", dn_outer, 3),
    )
    only(
        outer, ("ous3", up_swap, 3, late), ("ofx", from_x, 2, 0), ("ofx", from_x, 2, 1),
        ("ous2", up_swap, 2, early), ("oarr", arrive, 3, 0), ("oarr", arrive, 3, 1),
        ("ous2", up_swap, 2, late), ("dn", dn_outer, 0),
    )
    halves("fx", from_x, 3)
    for d in range(Z):
        run("norm", norm, d)
    forward(0)
    only(outer, ("dn", dn_outer, 1))
    run("usd", up_ready)
    only(outer, ("dn", dn_outer, 2))
    for d in range(Z):
        run("up", up, d)
    forward(1)
    only(outer, ("dn", dn_outer, 3))
    for c in range(C):
        run("ready", dn_ready, c)
        for k in (2, 3, 1, 0):
            run("down", down, c, k)
        if c > 0:
            run("side", to_side, c - 1)
        for k in (2, 3):
            run("x", over_x, c, k)
        for i in range(C - 2 if c == C - 1 else c, c + 1):
            if c != C - 2:
                for k in (1, 0):
                    run("x", over_x, i, k)
        if c + 2 < C:
            forward(c + 2)
        if c > 0:
            if c < C - 1:
                run("mate", to_mate, c - 1)
            run("across", across, c - 1)
    run("side", to_side, C - 1)
    run("fin", finish, 0)
    run("mate", to_mate, C - 2)
    for c in range(1, C - 2):
        run("fin", finish, c)
    run("across", across, C - 1)
    run("mate", to_mate, C - 1)
    run("fin", finish, C - 2)
    for c in range(C - 2):
        run("spread", spread, c)
    run("fin", finish, C - 1)
    for c in range(C - 2):
        run("coll", collect, c)
    for c in (C - 2, C - 1):
        run("spread", spread, c)
    for c in (C - 2, C - 1):
        run("coll", collect, c)
    with jax.named_scope("drain"):
        drain()


def fused(mesh_shape, tokens, mix_gain, group_weight, group_scale, mlp_gain, up_weight, up_scale, down_weight, down_scale):
    Z, T = mesh_shape["fs"], mesh_shape["tp"]
    C = CHUNKS
    rows, D = tokens.shape
    own = group_weight.shape[1]
    hg, hu = group_weight.shape[0] // 2, up_weight.shape[0] // 2
    fsub = up_weight.shape[1] // Z
    hd = fsub // 2
    dsub = down_weight.shape[1]
    cw = dsub // C
    bf, f32 = jnp.bfloat16, jnp.float32
    dma = pltpu.SemaphoreType.DMA
    vm = pl.BlockSpec(memory_space=pltpu.VMEM)
    hbm = pl.BlockSpec(memory_space=pltpu.HBM)
    sizes = (Z, T, C, rows, D, own, hg, hu, hd, fsub, dsub)
    V = pltpu.VMEM
    H = rows // LENGTH
    piece = (C, Z, rows, cw)
    pin = functools.partial(pltpu.with_memory_space_constraint, memory_space=pltpu.HBM)
    return pl.pallas_call(
        functools.partial(ring_kernel, sizes),
        out_shape=jax.ShapeDtypeStruct((rows, D), bf),
        in_specs=[hbm] * 9,
        out_specs=vm,
        scratch_shapes=[
            V((1, D), f32), V((1, own), f32), V((1, D), f32), V((1, Z * fsub), f32), V((1, D), f32),
            V((rows, D), bf), V((2 * hg, own), f32),
            V((Z, hu, fsub), f32), V((hu, fsub), f32), V((Z, hd, dsub), f32), V((hd, dsub), f32),
            V((Z * 2 * hg, own), bf), V((Z, hu, fsub), bf), V((Z * 2 * hu, fsub), bf),
            V((Z, C, hd, cw), bf), V((C, 2 * hd, Z * cw), bf),
            V((Z, T, rows, own), bf), V((Z, rows, D), bf), V((Z, rows, fsub), bf), V((C, Z, T, rows, cw), bf),
            V((C, Z, 2, rows, cw), bf), V(piece, bf), V(piece, bf), V(piece, bf), V((C, rows, cw), bf),
            V((C, 2, rows, cw), bf),
            dma((9 + 2 * Z,)), dma((13,)), dma((3,)), dma((1,)), dma((3, PARTS)), dma((1,)), dma((3, C)), dma((C,)),
            dma((Z, H)), dma((Z, H)), dma((Z,)), dma((C, Z)), dma((C,)), dma((C, Z)), dma((C, 2)), dma((C,)),
            dma((C,)), dma((C,)),
        ],
        compiler_params=pltpu.CompilerParams(
            collective_id=0, has_side_effects=True, vmem_limit_bytes=48000 * 1024
        ),
    )(
        *(pin(a) for a in (
            tokens, mix_gain[None], group_weight, group_scale, mlp_gain[None],
            up_weight, up_scale, down_weight, down_scale,
        ))
    )


def fits(mesh):
    shape = mesh.shape
    return shape["rep"] == 2 and shape["tp"] == GROUPS and shape["fs"] == shape["tp"]


def solution(mesh):
    in_specs = (
        P(("rep", "fs"), None),
        P(),
        P("fs", "tp"),
        P(None, "tp"),
        P(),
        P("fs", "tp"),
        P(None, "tp"),
        P("tp", "fs"),
        P(),
    )
    out_specs = P(("rep", "fs"), None)
    chosen = functools.partial(fused, mesh.shape) if fits(mesh) else body
    return jax.shard_map(chosen, mesh=mesh, in_specs=in_specs, out_specs=out_specs, check_vma=False)
```

```python
import functools

import jax
import jax.numpy as jnp
from jax import lax
from jax.experimental import pallas as pl
from jax.experimental.pallas import tpu as pltpu
from jax.sharding import PartitionSpec as P

GROUPS = 4
LENGTH = 128


norm_eps = 1e-06


def norm_rows(values, gain):
    promoted = values.astype(jnp.float32)
    inverse = lax.rsqrt(jnp.mean(promoted * promoted, axis=-1, keepdims=True) + norm_eps)
    return (promoted * inverse * gain).astype(jnp.bfloat16)


def band_means(inputs, window, seq_length):
    row_count, columns = inputs.shape
    by_sequence = inputs.reshape(row_count // seq_length, seq_length, columns)
    position = jnp.arange(seq_length, dtype=jnp.int32)
    offset = position[:, None] - position[None, :]
    band_mask = ((offset >= 0) & (offset < window)).astype(jnp.bfloat16)
    divisor = jnp.minimum(position + 1, window).astype(jnp.float32)
    summed = jnp.einsum("ts,nsc->ntc", band_mask, by_sequence, preferred_element_type=jnp.float32)
    return (summed / divisor[None, :, None] - by_sequence.astype(jnp.float32)).reshape(
        row_count, columns
    )


def body(
    tokens,
    mix_gain,
    group_weight,
    group_scale,
    mlp_gain,
    up_weight,
    up_scale,
    down_weight,
    down_scale,
):
    model_width = tokens.shape[1]
    group_width = model_width // GROUPS
    own_cols = group_weight.shape[1]
    column_start = lax.axis_index("tp") * own_cols
    group_index = column_start // group_width
    normed = norm_rows(tokens, mix_gain)
    inputs = lax.dynamic_slice_in_dim(normed, group_index * group_width, group_width, 1)
    window = jnp.left_shift(jnp.int32(2), group_index)
    pooled = band_means(inputs, window, LENGTH).astype(jnp.bfloat16)
    mixed_cols = (
        jnp.dot(
            pooled,
            lax.all_gather(group_weight.astype(jnp.bfloat16), "fs", axis=0, tiled=True),
            preferred_element_type=jnp.float32,
        )
        * group_scale
    )
    own_tokens = lax.dynamic_slice_in_dim(tokens, column_start, own_cols, 1)
    carried_cols = (own_tokens.astype(jnp.float32) + mixed_cols).astype(jnp.bfloat16)
    carried = lax.all_gather(carried_cols, "tp", axis=1, tiled=True)
    normed_mlp = norm_rows(carried, mlp_gain)
    pre_act = (
        jnp.dot(
            normed_mlp,
            lax.all_gather(up_weight.astype(jnp.bfloat16), "fs", axis=0, tiled=True),
            preferred_element_type=jnp.float32,
        )
        * up_scale
    )
    hidden = jnp.square(jax.nn.relu(pre_act)).astype(jnp.bfloat16)
    partial_value = (
        jnp.dot(
            hidden,
            lax.all_gather(down_weight.astype(jnp.bfloat16), "fs", axis=1, tiled=True),
            preferred_element_type=jnp.float32,
        )
        * down_scale
    )
    summed = lax.psum(partial_value.astype(jnp.bfloat16), "tp").astype(jnp.float32)
    return (carried.astype(jnp.float32) + summed).astype(jnp.bfloat16)


MESH = pl.DeviceIdType.MESH
CHUNKS = 4
PARTS = 4


def ring_kernel(
    sizes,
    tok_h, mg_h, gw_h, gs_h, lg_h, up_h, us_h, dn_h, ds_h,
    out_h,
    mg, gs, lg, us, ds,
    tok, gwf, upf, upo, dnf, dno,
    gwg, ups, upg, dns, dng,
    car, xn, hid, pb, ra, sx, rb, sz, ri, rc,
    ld, sent, rw, ry, rwu, ryu, rwd, ryd, rcz, rcx, rcc, rx, rj, rb_s, rt, rm, ro, rq,
):
    Z, T, C, rows, D, own, hg, hu, hd, fsub, dsub = sizes
    cw = dsub // C
    r, z, t = lax.axis_index("rep"), lax.axis_index("fs"), lax.axis_index("tp")
    cp = t + 1 - 2 * lax.rem(t, 2)
    xp = lax.rem(t + 2, T)
    cxp = lax.rem(cp + 2, T)
    peer_r = 1 - r
    bf, f32 = jnp.bfloat16, jnp.float32
    mate = z + 1 - 2 * lax.rem(z, 2)
    zk = (z, mate, lax.rem(z + 2, Z), Z - 1 - z)
    inner = (z > 0) & (z < Z - 1)
    outer = (z == 0) | (z == Z - 1)

    def mul(i, n):
        return pl.multiple_of(i * n, n)

    loads = {}

    def load(key, src, dst, k):
        c = pltpu.make_async_copy(src, dst, ld.at[k])
        c.start()
        loads[key] = c

    def load_up(k):
        load(("up", k), up_h.at[pl.ds(mul(r, hu), hu), pl.ds(mul(zk[k], fsub), fsub)], upf.at[k], 2 + k)

    def load_dn(k):
        load(("dn", k), dn_h.at[pl.ds(pl.multiple_of(zk[k] * 2 * hd + r * hd, hd), hd), :], dnf.at[k], 2 + Z + k)

    load("gw", gw_h, gwf, 0)
    load_up(2)
    load("tok", tok_h, tok, 1)
    load_up(3)
    load_up(1)
    load_up(0)
    load("upo", up_h.at[pl.ds(mul(peer_r, hu), hu), pl.ds(mul(z, fsub), fsub)], upo, 2 + 2 * Z)
    for k in (2, 3, 1, 0):
        load_dn(k)
    small = (("mg", mg_h, mg), ("gs", gs_h, gs), ("lg", lg_h, lg), ("us", us_h, us), ("ds", ds_h, ds))
    for i, (key, src, dst) in enumerate(small):
        load(key, src, dst, 4 + 2 * Z + i)
    load("dno", dn_h.at[pl.ds(pl.multiple_of(z * 2 * hd + peer_r * hd, hd), hd), :], dno, 3 + 2 * Z)

    barrier = pltpu.get_barrier_semaphore()
    peers = [(r, zk[k], t) for k in range(1, Z)] + [(peer_r, z, t), (r, z, xp), (r, z, cp)]
    for p in peers:
        pl.semaphore_signal(barrier, inc=1, device_id=p, device_id_type=MESH)
    loads["gw"].wait()
    gwg[pl.ds(mul(z, 2 * hg), 2 * hg), :] = gwf[...].astype(bf)
    loads[("up", 2)].wait()
    ups[2] = upf[2].astype(bf)
    with jax.named_scope("barrier"):
        pl.semaphore_wait(barrier, len(peers))

    def remote(src, dst, ss, rs, dev):
        return pltpu.make_async_remote_copy(
            src_ref=src, dst_ref=dst, send_sem=ss, recv_sem=rs, device_id=dev, device_id_type=MESH
        )

    role = [None]

    def guarded(fn, when=None):
        for p in (role[0],):
            if p is not None:
                when = p if when is None else when & p
        if when is None:
            fn()
        else:
            pl.when(when)(fn)
        return when

    groups = ("gw", "gwy", "up", "upy", "dn", "dny", "carz", "carx", "carc", "pb", "sx", "sz", "og")

    def send(src, dst, group, rs, dev, when=None):
        guarded(lambda: remote(src, dst, sent.at[groups.index(group)], rs, dev).start(), when)

    def drain():
        three = pl.ds(1, Z - 1)
        same = (
            gwg.at[pl.ds(0, (Z - 1) * hg)], gwg.at[pl.ds(0, (Z - 1) * hg)], ups.at[three], ups.at[three],
            dns.at[three], dns.at[three], car.at[0, three], car.at[0], car.at[pl.ds(0, 2)],
            ra, rb, sx.at[:, three], sx.at[:, three],
        )
        for i, ref in enumerate(same):
            remote(ref, ref, sent.at[i], rcc.at[0], (peer_r, z, t)).wait_send()

    def got(dst, rs):
        guarded(lambda: remote(dst, dst, sent.at[0], rs, (peer_r, z, t)).wait_recv())

    def only(who, *steps):
        role[0] = who
        for name, fn, *args in steps:
            run(name, fn, *args)
        role[0] = None

    def run(name, fn, *args):
        with jax.named_scope(name + "".join(map(str, [a for a in args if isinstance(a, int)]))):
            fn(*args)

    def gw_at(src, rep):
        return gwg.at[pl.ds(pl.multiple_of(src * 2 * hg + rep * hg, hg), hg), :]

    pu = hu // PARTS

    def up_at(src, rep, i):
        return upg.at[pl.ds(pl.multiple_of(src * 2 * hu + rep * hu + i * pu, pu), pu), :]

    def dn_at(c, src, rep):
        return dng.at[c, pl.ds(mul(rep, hd), hd), pl.ds(mul(src, cw), cw)]

    early, late = range(PARTS // 2), range(PARTS // 2, PARTS)
    whole = range(PARTS)

    def up_send(k, when=None, parts=whole):
        for i in parts:
            piece = ups.at[k, pl.ds(i * pu, pu)]
            send(piece, up_at(z, r, i), "up", rwu.at[k - 1, i], (r, zk[k], t), when)

    def dn_send(c, k):
        send(dns.at[k, c], dn_at(c, z, r), "dn", rwd.at[k - 1, c], (r, zk[k], t))

    for k in (3, 2, 1):
        send(gw_at(z, r), gw_at(z, r), "gw", rw.at[k - 1], (r, zk[k], t))
    loads[("up", 1)].wait()
    ups[1] = upf[1].astype(bf)
    loads[("up", 3)].wait()
    ups[3] = upf[3].astype(bf)
    up_send(1, None, early)
    up_send(1, inner, late)

    for key in ("tok", "mg", "gs", "lg", "us", "ds"):
        loads[key].wait()
    full = tok[...].astype(f32)
    inv = lax.rsqrt(jnp.mean(full * full, axis=-1, keepdims=True) + norm_eps)
    cols = pl.ds(mul(t, own), own)
    mine = tok[:, cols].astype(f32)
    normed = (mine * inv * mg[:, cols]).astype(bf)
    window = jnp.left_shift(jnp.int32(2), t)
    ti = lax.broadcasted_iota(jnp.int32, (LENGTH, LENGTH), 0)
    si = lax.broadcasted_iota(jnp.int32, (LENGTH, LENGTH), 1)
    band = jnp.where((ti - si >= 0) & (ti - si < window), 1.0, 0.0).astype(bf)
    pos = lax.broadcasted_iota(jnp.int32, (LENGTH, own), 0)
    divisor = jnp.minimum(pos + 1, window).astype(f32)
    for s in range(rows // LENGTH):
        part = normed[s * LENGTH:(s + 1) * LENGTH]
        summed = jnp.dot(band, part, preferred_element_type=f32)
        xn[0, s * LENGTH:(s + 1) * LENGTH, :own] = (summed / divisor - part.astype(f32)).astype(bf)

    def gw_swap(k):
        b = gw_at(zk[k], r)
        got(b, rw.at[k - 1])
        send(b, b, "gwy", ry.at[0], (peer_r, z, t))

    def up_swap(k, parts=whole):
        for i in parts:
            b = up_at(zk[k], r, i)
            got(b, rwu.at[k - 1, i])
            send(b, b, "upy", ryu.at[0], (peer_r, z, t))

    up_send(2, inner, early)
    with jax.named_scope("gwswap"):
        for k in (1, 2, 3):
            gw_swap(k)
        up_send(3, outer, early)
        up_send(2, outer, early)
    with jax.named_scope("gwswapped"):
        got(gwg.at[pl.ds(0, (Z - 1) * hg)], ry.at[0])
    with jax.named_scope("mix"):
        mixed = jnp.dot(xn[0, :, :own], gwg[...], preferred_element_type=f32) * gs[...]
        car[z, t] = (tok[:, cols].astype(f32) + mixed).astype(bf)
    H = rows // LENGTH
    hr = LENGTH
    is_in = lax.rem(lax.div(z + 1, 2), 2)
    blocks = (z, is_in * zk[1] + (1 - is_in) * zk[3], is_in * zk[3] + (1 - is_in) * zk[1], zk[2])

    def half(h):
        return pl.ds(h * hr, hr)

    def to_x(src, h):
        b = car.at[src, t, half(h)]
        send(b, b, "carx", rcx.at[src, h], (r, z, xp))

    def to_core(src, h, q):
        b = car.at[src, q, half(h)]
        send(b, b, "carc", rcc.at[src], (r, z, cp))

    def to_z(src, h, dev, when=None):
        b = car.at[src, t, half(h)]
        send(b, b, "carz", rcz.at[src, h], (r, dev, t), when)

    for h in range(H):
        to_z(z, h, zk[3])
        to_z(z, h, mate)
        to_x(z, h)
        to_core(z, h, t)
    up_send(3, inner, early)
    for parts in (late,):
        up_send(2, inner, parts)
        up_send(3, inner, parts)

    with jax.named_scope("casts"):
        for k in (2, 3, 1):
            loads[("dn", k)].wait()
            for c in range(C):
                dns[k, c] = dnf[k, :, c * cw:(c + 1) * cw].astype(bf)
        loads[("up", 0)].wait()
        upg[pl.ds(pl.multiple_of(z * 2 * hu + r * hu, hu), hu), :] = upf[0].astype(bf)
        loads["upo"].wait()
        upg[pl.ds(pl.multiple_of(z * 2 * hu + peer_r * hu, hu), hu), :] = upo[...].astype(bf)
        loads[("dn", 0)].wait()
        loads["dno"].wait()
        for c in range(C):
            here = pl.ds(mul(z, cw), cw)
            dng[c, pl.ds(mul(r, hd), hd), here] = dnf[0, :, c * cw:(c + 1) * cw].astype(bf)
            dng[c, pl.ds(mul(peer_r, hd), hd), here] = dno[:, c * cw:(c + 1) * cw].astype(bf)

    def arrive(d, h):
        src = blocks[d]
        got(car.at[src, t, half(h)], rcz.at[src, h])
        if d < 3:
            to_z(src, h, mate, outer if d == 1 else inner)
        to_x(src, h)
        to_core(src, h, t)

    def from_x(d, h):
        src = blocks[d]
        got(car.at[src, xp, half(h)], rcx.at[src, h])
        to_core(src, h, xp)

    def dn_group(*pieces):
        for c, k in pieces:
            dn_send(c, k)

    def dn_outer(c):
        dn_group((c, 3), (c, 2), (c, 1))

    def dn_forward(c, k):
        src = zk[k]
        got(dn_at(c, src, r), rwd.at[k - 1, c])
        send(dn_at(c, src, r), dn_at(c, src, r), "dny", ryd.at[c], (peer_r, z, t))

    def norm(d):
        src = blocks[d]
        got(car.at[src, pl.ds(0, 2)], rcc.at[src])
        total = jnp.zeros((rows, 1), f32)
        for q in range(T):
            c = car[src, q].astype(f32)
            total += jnp.sum(c * c, axis=-1, keepdims=True)
        scale = lax.rsqrt(total / D + norm_eps)
        for q in range(T):
            part = slice(q * own, (q + 1) * own)
            xn[d, :, part] = (car[src, q].astype(f32) * scale * lg[:, part]).astype(bf)

    def up(d):
        pre = jnp.dot(xn[d], upg[...], preferred_element_type=f32)
        pre = jnp.maximum(pre * us[:, pl.ds(mul(z, fsub), fsub)], 0.0)
        hid[blocks[d]] = (pre * pre).astype(bf)

    def dn_ready(c):
        got(dns.at[0, pl.ds(0, Z - 1)], ryd.at[c])

    def down(c, k):
        src = zk[k]
        p = jnp.dot(hid[src], dng[c], preferred_element_type=f32)
        for q in range(T):
            part = p[:, q * cw:(q + 1) * cw] * ds[:, q * own + c * cw:q * own + (c + 1) * cw]
            pb[c, src, q] = part.astype(bf)
        for j, q in ((1, cxp), (0, cp)):
            send(pb.at[c, src, q], ra.at[c, src, j], "pb", rx.at[c, src] if j else rj.at[c], (r, z, cp))

    def over_x(c, k):
        src = zk[k]
        got(ra.at[c, src, 1], rx.at[c, src])
        sx[c, src] = (pb[c, src, xp].astype(f32) + ra[c, src, 1].astype(f32)).astype(bf)
        send(sx.at[c, src], rb.at[c, src], "sx", rb_s.at[c, src], (r, z, xp))

    def both(c, src):
        return pb[c, src, t].astype(f32) + ra[c, src, 0].astype(f32) + rb[c, src].astype(f32)

    def joined(c, k):
        src = zk[k]
        if k == 2:
            got(sx.at[c], rj.at[c])
        got(rb.at[c, src], rb_s.at[c, src])

    def to_side(c):
        src = zk[2]
        joined(c, 2)
        sz[c, src] = both(c, src).astype(bf)
        send(sz.at[c, src], ri.at[c], "sz", rm.at[c], (r, mate, t))

    def across(c):
        src = zk[3]
        joined(c, 3)
        got(ri.at[c], rm.at[c])
        sz[c, src] = (both(c, src) + ri[c].astype(f32)).astype(bf)
        send(sz.at[c, src], rc.at[c, 1], "sz", rt.at[c, 1], (r, src, t))

    def to_mate(c):
        joined(c, 1)
        sz[c, mate] = both(c, mate).astype(bf)
        send(sz.at[c, mate], rc.at[c, 0], "sz", rt.at[c, 0], (r, mate, t))

    def og(c, q):
        return out_h.at[:, pl.ds(pl.multiple_of(q * own + c * cw, cw), cw)]

    def pass_on(c, q, rs, dev):
        send(og(c, q), og(c, q), "og", rs, dev)

    def finish(c):
        joined(c, 0)
        acc = both(c, z) + car[z, t, :, :].astype(f32)[:, c * cw:(c + 1) * cw]
        for j in range(2):
            got(rc.at[c, j], rt.at[c, j])
            acc += rc[c, j].astype(f32)
        out_h[:, pl.ds(pl.multiple_of(t * own + c * cw, cw), cw)] = acc.astype(bf)
        pass_on(c, t, ro.at[c], (r, z, xp))
        pass_on(c, t, rq.at[c], (r, z, cp))

    def spread(c):
        got(og(c, xp), ro.at[c])
        pass_on(c, xp, rq.at[c], (r, z, cp))

    def collect(c):
        got(sx.at[c, pl.ds(0, 2)], rq.at[c])

    def up_ready():
        got(ups.at[pl.ds(0, Z - 1)], ryu.at[0])

    def forward(c):
        for k in (1, 2, 3):
            run("fwd", dn_forward, c, k)

    def halves(name, fn, d):
        for h in range(H):
            run(name, fn, d, h)

    only(outer, ("ous3", up_swap, 3, early))
    only(inner, ("ius1", up_swap, 1, early), ("ius2", up_swap, 2, early))
    halves("fx", from_x, 0)
    halves("arr", arrive, 1)
    only(
        outer, ("ou2", up_send, 2, None, late), ("ou3", up_send, 3, None, late), ("ou1", up_send, 1, None, late),
        ("ous1", up_swap, 1), ("ofx", from_x, 1, 0), ("ofx", from_x, 1, 1),
    )
    halves("arr", arrive, 2)
    only(
        inner, ("ifx", from_x, 1, 0), ("ifx", from_x, 1, 1), ("iarr", arrive, 3, 0), ("iarr", arrive, 3, 1),
        ("dn", dn_outer, 0), ("dn", dn_outer, 1),
        ("ius2", up_swap, 2, late), ("ius1", up_swap, 1, late),
        ("ifx", from_x, 2, 0), ("ifx", from_x, 2, 1),
        ("ius3", up_swap, 3), ("dn", dn_outer, 2), ("dn", dn_outer, 3),
    )
    only(
        outer, ("ous3", up_swap, 3, late), ("ofx", from_x, 2, 0), ("ofx", from_x, 2, 1),
        ("ous2", up_swap, 2, early), ("oarr", arrive, 3, 0), ("oarr", arrive, 3, 1),
        ("ous2", up_swap, 2, late), ("dn", dn_outer, 0),
    )
    halves("fx", from_x, 3)
    for d in range(Z):
        run("norm", norm, d)
    forward(0)
    only(outer, ("dn", dn_outer, 1))
    run("usd", up_ready)
    only(outer, ("dn", dn_outer, 2))
    for d in range(Z):
        run("up", up, d)
    forward(1)
    only(outer, ("dn", dn_outer, 3))
    for c in range(C):
        run("ready", dn_ready, c)
        for k in (2, 3, 1, 0):
            run("down", down, c, k)
        if c > 0:
            run("side", to_side, c - 1)
        for k in (2, 3):
            run("x", over_x, c, k)
        for i in range(C - 2 if c == C - 1 else c, c + 1):
            if c != C - 2:
                for k in (1, 0):
                    run("x", over_x, i, k)
        if c + 2 < C:
            forward(c + 2)
        if c > 0:
            if c < C - 1:
                run("mate", to_mate, c - 1)
            run("across", across, c - 1)
    run("side", to_side, C - 1)
    run("fin", finish, 0)
    run("mate", to_mate, C - 2)
    for c in range(1, C - 2):
        run("fin", finish, c)
    run("across", across, C - 1)
    run("mate", to_mate, C - 1)
    run("fin", finish, C - 2)
    for c in range(C - 2):
        run("spread", spread, c)
    run("fin", finish, C - 1)
    for c in range(C - 2):
        run("coll", collect, c)
    for c in (C - 2, C - 1):
        run("spread", spread, c)
    for c in (C - 2, C - 1):
        run("coll", collect, c)
    with jax.named_scope("drain"):
        drain()


def fused(mesh_shape, tokens, mix_gain, group_weight, group_scale, mlp_gain, up_weight, up_scale, down_weight, down_scale):
    Z, T = mesh_shape["fs"], mesh_shape["tp"]
    C = CHUNKS
    rows, D = tokens.shape
    own = group_weight.shape[1]
    hg, hu = group_weight.shape[0] // 2, up_weight.shape[0] // 2
    fsub = up_weight.shape[1] // Z
    hd = fsub // 2
    dsub = down_weight.shape[1]
    cw = dsub // C
    bf, f32 = jnp.bfloat16, jnp.float32
    dma = pltpu.SemaphoreType.DMA
    vm = pl.BlockSpec(memory_space=pltpu.VMEM)
    hbm = pl.BlockSpec(memory_space=pltpu.HBM)
    sizes = (Z, T, C, rows, D, own, hg, hu, hd, fsub, dsub)
    V = pltpu.VMEM
    H = rows // LENGTH
    piece = (C, Z, rows, cw)
    pin = functools.partial(pltpu.with_memory_space_constraint, memory_space=pltpu.HBM)
    return pl.pallas_call(
        functools.partial(ring_kernel, sizes),
        out_shape=jax.ShapeDtypeStruct((rows, D), bf),
        in_specs=[hbm] * 9,
        out_specs=vm,
        scratch_shapes=[
            V((1, D), f32), V((1, own), f32), V((1, D), f32), V((1, Z * fsub), f32), V((1, D), f32),
            V((rows, D), bf), V((2 * hg, own), f32),
            V((Z, hu, fsub), f32), V((hu, fsub), f32), V((Z, hd, dsub), f32), V((hd, dsub), f32),
            V((Z * 2 * hg, own), bf), V((Z, hu, fsub), bf), V((Z * 2 * hu, fsub), bf),
            V((Z, C, hd, cw), bf), V((C, 2 * hd, Z * cw), bf),
            V((Z, T, rows, own), bf), V((Z, rows, D), bf), V((Z, rows, fsub), bf), V((C, Z, T, rows, cw), bf),
            V((C, Z, 2, rows, cw), bf), V(piece, bf), V(piece, bf), V(piece, bf), V((C, rows, cw), bf),
            V((C, 2, rows, cw), bf),
            dma((9 + 2 * Z,)), dma((13,)), dma((3,)), dma((1,)), dma((3, PARTS)), dma((1,)), dma((3, C)), dma((C,)),
            dma((Z, H)), dma((Z, H)), dma((Z,)), dma((C, Z)), dma((C,)), dma((C, Z)), dma((C, 2)), dma((C,)),
            dma((C,)), dma((C,)),
        ],
        compiler_params=pltpu.CompilerParams(
            collective_id=0, has_side_effects=True, vmem_limit_bytes=48000 * 1024
        ),
    )(
        *(pin(a) for a in (
            tokens, mix_gain[None], group_weight, group_scale, mlp_gain[None],
            up_weight, up_scale, down_weight, down_scale,
        ))
    )


def fits(mesh):
    shape = mesh.shape
    return shape["rep"] == 2 and shape["tp"] == GROUPS and shape["fs"] == shape["tp"]


def solution(mesh):
    in_specs = (
        P(("rep", "fs"), None),
        P(),
        P("fs", "tp"),
        P(None, "tp"),
        P(),
        P("fs", "tp"),
        P(None, "tp"),
        P("tp", "fs"),
        P(),
    )
    out_specs = P(("rep", "fs"), None)
    chosen = functools.partial(fused, mesh.shape) if fits(mesh) else body
    return jax.shard_map(chosen, mesh=mesh, in_specs=in_specs, out_specs=out_specs, check_vma=False)
```
